32 devices in a mesh: dp: 4 (over y, x), kv: 4 (over z), tp: 2 (over core).
Axes of the slice: x: 2, y: 2, z: 4, core: 2. Of those that a mesh axis runs over, the one named last changes fastest.
Arguments:
- tokens: bfloat16 [16, 4096], P('dp', ('kv', 'tp')), may hold values from -24 to 24
- rec_state: float32 [16, 16, 128, 128], P(('dp', 'kv'), 'tp'), may hold values from -2 to 2
- norm_gain: float32 [4096], replicated, may hold values from 0.1 to 1.9
- w_query: bfloat16 [4096, 2048], P('kv', 'tp'), may hold values from -0.09375 to 0.09375
- w_forget: bfloat16 [4096, 2048], P('kv', 'tp'), may hold values from -0.09375 to 0.09375
- w_input: bfloat16 [4096, 2048], P('kv', 'tp'), may hold values from -0.09375 to 0.09375
- w_outgate: bfloat16 [4096, 2048], P('kv', 'tp'), may hold values from -0.09375 to 0.09375
- lower_bound: float32 [2048], P('tp'), may hold values from 0 to 0.9
- head_gain: float32 [2048], P('tp'), may hold values from 0.1 to 1.9
- w_heads_out: bfloat16 [2048, 4096], P(None, ('kv', 'tp')), may hold values from -0.125 to 0.125
- mixer_gain: float32 [4096], replicated, may hold values from 0.1 to 1.9
- w_gate: bfloat16 [4096, 11264], P(None, ('kv', 'tp')), may hold values from -0.09375 to 0.09375
- w_up: bfloat16 [4096, 11264], P(None, ('kv', 'tp')), may hold values from -0.09375 to 0.09375
- w_down: bfloat16 [11264, 4096], P(('kv', 'tp')), may hold values from -0.078125 to 0.078125
Outputs:
- result: bfloat16 [16, 4096], P('dp', ('kv', 'tp'))
- new_state: float32 [16, 16, 128, 128], P(('dp', 'kv'), 'tp')
The draws below stay inside these ranges and needn't reach their ends.
All inputs are finite; a program needn't handle non-finite values.
Results may differ from the reference program's by a relative error of at most 0.012.
Values may be sent and summed in bfloat16 or wider, within the bound.
No kernel may reach another device: no remote copies, remote signals or barrier semaphores. Data moves between devices by JAX's collectives and lax.ppermute only.
A program may use at most 128 MiB of HBM per device.

```python
import math
import jax
import jax.numpy as jnp
from jax import lax

D = 4096
HEAD_DIM = 128
HEADS = 16
FF = 11264
HG = 2048
BATCH = 16


def draw_tokens(key, part):
    key_rows = jax.random.fold_in(key, 11)
    key_vals = jax.random.fold_in(key, 12)
    col_scale = jnp.exp(jnp.linspace(math.log(0.5), math.log(2.0), D))[None, :]
    row_scale = jnp.exp(jax.random.uniform(key_rows, (BATCH, 1), jnp.float32, math.log(0.3), math.log(3.0)))
    values = jnp.clip(jax.random.normal(key_vals, (BATCH, D), jnp.float32), -4.0, 4.0)
    return (values * row_scale * col_scale).astype(jnp.bfloat16)


def strengthened(array, own_key, source, target, parts, factor):
    owner, partner = [(jnp.arange(array.shape[dim]) // (array.shape[dim] // parts)).reshape([-1 if axis == dim else 1 for axis in range(array.ndim)]) for dim in (source, target)]
    chosen = jax.random.permutation(own_key, parts)[partner]
    strong = (owner == chosen) | (owner == (partner + parts // 2) % parts)
    return jnp.where(strong, factor * array, array)


def block_levels(rng, shape, shards, least, top_value):
    loudness = 1.0
    for axis_at, parts in shards:
        steps = jax.random.uniform(jax.random.fold_in(jax.random.fold_in(rng, 6), axis_at), (parts,), jnp.float32, least / len(shards), top_value / len(shards))
        loudness = loudness * jnp.repeat(jnp.exp(steps), shape[axis_at] // parts).reshape((-1,) + (1,) * (len(shape) - 1 - axis_at))
    return loudness


def gaussian(key, extent, deviation, limit, shards=(), kind=jnp.bfloat16):
    drawn = deviation * jax.random.normal(key, extent, jnp.float32)
    if shards:
        drawn = drawn * block_levels(key, extent, shards, -0.22, 0.18)
    return jnp.clip(drawn, -limit, limit).astype(kind)


def noise_with(stream_key, shape, scale, bound, split, heavy, held_as=jnp.bfloat16):
    array = scale * jax.random.normal(stream_key, shape, jnp.float32)
    if split:
        array = array * block_levels(stream_key, shape, split, -0.22, 0.18)
    return jnp.clip(strengthened(array, jax.random.fold_in(stream_key, 3), *heavy), -bound, bound).astype(held_as)


def setup_inputs(seed: int = 0) -> dict:
    streams_of = jax.random.split(jax.random.key(seed), 15)
    return {
        "tokens": draw_tokens(jax.random.fold_in(streams_of[14], 71), 0),
        "rec_state": gaussian(streams_of[1], (BATCH, HEADS, HEAD_DIM, HEAD_DIM), 0.3, 2.0, ((0, 16), (1, 2)), jnp.float32),
        "norm_gain": jnp.clip(1.0 + 0.18 * jax.random.normal(streams_of[2], (D,), jnp.float32), 0.1, 1.9),
        "w_query": gaussian(streams_of[3], (D, HG), D ** -0.5, 0.09375, ((0, 4), (1, 2))),
        "w_forget": gaussian(streams_of[4], (D, HG), D ** -0.5, 0.09375, ((0, 4), (1, 2))),
        "w_input": gaussian(streams_of[5], (D, HG), D ** -0.5, 0.09375, ((0, 4), (1, 2))),
        "w_outgate": gaussian(streams_of[6], (D, HG), D ** -0.5, 0.09375, ((0, 4), (1, 2))),
        "lower_bound": jnp.clip(0.9 * jax.random.uniform(streams_of[7], (HG,), jnp.float32) ** block_levels(streams_of[7], (HG,), ((0, 2),), -0.2, 0.2), 0.0, 0.9),
        "head_gain": jnp.clip(1.0 + 0.18 * jax.random.normal(streams_of[8], (HG,), jnp.float32), 0.1, 1.9),
        "w_heads_out": gaussian(streams_of[9], (HG, D), HG ** -0.5, 0.125, ((1, 8),)),
        "mixer_gain": jnp.clip(1.0 + 0.18 * jax.random.normal(streams_of[10], (D,), jnp.float32), 0.1, 1.9),
        "w_gate": gaussian(streams_of[11], (D, FF), D ** -0.5, 0.09375, ((1, 8),)),
        "w_up": gaussian(streams_of[12], (D, FF), D ** -0.5, 0.09375, ((1, 8),)),
        "w_down": noise_with(streams_of[13], (FF, D), FF ** -0.5, 0.078125, ((0, 8),), (0, 1, 8, 2.0)),
    }


epsilon = 1e-06

def reference(tokens, rec_state, norm_gain, w_query, w_forget, w_input, w_outgate, lower_bound, head_gain, w_heads_out, mixer_gain, w_gate, w_up, w_down):
    tok_float = tokens.astype(jnp.float32)
    row_scale = lax.rsqrt(lax.optimization_barrier(jnp.mean(tok_float * tok_float, axis=1, keepdims=True)) + epsilon)
    scaled = (tok_float * norm_gain).astype(jnp.bfloat16)
    query_pre = row_scale * jnp.dot(scaled, w_query, preferred_element_type=jnp.float32)
    forget_pre = row_scale * jnp.dot(scaled, w_forget, preferred_element_type=jnp.float32)
    value_in = row_scale * jnp.dot(scaled, w_input, preferred_element_type=jnp.float32)
    gate_pre = row_scale * jnp.dot(scaled, w_outgate, preferred_element_type=jnp.float32)
    forget = lower_bound + (1.0 - lower_bound) * jax.nn.sigmoid(forget_pre)
    key_in = 1.0 - forget
    query_act = jax.nn.silu(query_pre)
    batch_rows = tokens.shape[0]
    shaped = (batch_rows, HEADS, HEAD_DIM)
    forget = forget.reshape(shaped)
    key_in = key_in.reshape(shaped)
    value_in = value_in.reshape(shaped)
    query_act = query_act.reshape(shaped)
    new_state = forget[:, :, :, None] * rec_state + key_in[:, :, :, None] * value_in[:, :, None, :]
    head_out = lax.optimization_barrier(jnp.sum(query_act[:, :, :, None] * new_state, axis=2))
    head_out = head_out * lax.rsqrt(lax.optimization_barrier(jnp.mean(head_out * head_out, axis=2, keepdims=True)) + epsilon)
    head_out = head_out * head_gain.reshape(HEADS, HEAD_DIM)
    gated = (head_out.reshape(batch_rows, HG) * jax.nn.silu(gate_pre)).astype(jnp.bfloat16)
    mixed = (tok_float + jnp.dot(gated, w_heads_out, preferred_element_type=jnp.float32)).astype(jnp.bfloat16)
    mixed_float = mixed.astype(jnp.float32)
    mixer_scale = lax.rsqrt(lax.optimization_barrier(jnp.mean(mixed_float * mixed_float, axis=1, keepdims=True)) + epsilon)
    normed = (mixed_float * mixer_scale * mixer_gain).astype(jnp.bfloat16)
    gate_val = jnp.dot(normed, w_gate, preferred_element_type=jnp.float32)
    up_val = jnp.dot(normed, w_up, preferred_element_type=jnp.float32)
    hidden = (jax.nn.silu(gate_val) * up_val).astype(jnp.bfloat16)
    result = (mixed_float + jnp.dot(hidden, w_down, preferred_element_type=jnp.float32)).astype(jnp.bfloat16)
    return (result, new_state)
```

```python
import jax
import jax.numpy as jnp
from jax import lax
from jax.sharding import PartitionSpec as P

HEAD_DIM = 128


epsilon = 1e-06
GROUP = ("kv", "tp")


def channel_mixer(whole_rows, mixer_gain, w_gate, w_up, w_down):
    rows_float = whole_rows.astype(jnp.float32)
    mixer_scale = lax.rsqrt(jnp.mean(rows_float * rows_float, axis=1, keepdims=True) + epsilon)
    normed = (rows_float * mixer_scale * mixer_gain).astype(jnp.bfloat16)
    gate_val = jnp.dot(normed, w_gate, preferred_element_type=jnp.float32)
    up_val = jnp.dot(normed, w_up, preferred_element_type=jnp.float32)
    hidden = (jax.nn.silu(gate_val) * up_val).astype(jnp.bfloat16)
    return jnp.dot(hidden, w_down, preferred_element_type=jnp.float32)


def gather_group(block, count):
    copies = jnp.broadcast_to(block[None], (count,) + block.shape)
    return lax.all_to_all(copies, GROUP, 0, 0)


def local(
    tokens,
    rec_state,
    norm_gain,
    w_query,
    w_forget,
    w_input,
    w_outgate,
    lower_bound,
    head_gain,
    w_heads_out,
    mixer_gain,
    w_gate,
    w_up,
    w_down,
):
    kv_count = lax.axis_size("kv")
    tp_count = lax.axis_size("tp")
    kv_index = lax.axis_index("kv")
    tp_index = lax.axis_index("tp")
    group_count = kv_count * tp_count
    row_count = tokens.shape[0]
    seq_count = rec_state.shape[0]
    model_width = norm_gain.shape[0]
    col_block = model_width // kv_count
    tok_float = tokens.astype(jnp.float32)
    other = lax.ppermute(tokens, "tp", [(i, (i + 1) % tp_count) for i in range(tp_count)])
    low = jnp.where(tp_index == 0, tokens, other)
    high = jnp.where(tp_index == 0, other, tokens)
    own_cols = jnp.concatenate([low, high], axis=1).astype(jnp.float32)
    squares = jnp.sum(own_cols * own_cols, axis=1)
    gain_block = lax.dynamic_slice_in_dim(norm_gain, kv_index * col_block, col_block, 0)
    scaled = (own_cols * gain_block).astype(jnp.bfloat16)
    partial = [
        jnp.dot(scaled, weight, preferred_element_type=jnp.float32)
        for weight in (w_query, w_forget, w_input, w_outgate)
    ]
    local_width = w_query.shape[1]
    partial.append(jnp.broadcast_to(squares[:, None], (row_count, 128)))
    sent = jnp.concatenate(partial, axis=1).reshape(kv_count, seq_count, -1)
    projected = jnp.sum(lax.all_to_all(sent, "kv", 0, 0), axis=0)
    my_squares = projected[:, 4 * local_width]
    row_scale = lax.rsqrt(my_squares / model_width + epsilon)[:, None]
    query_pre = row_scale * projected[:, :local_width]
    forget_pre = row_scale * projected[:, local_width : 2 * local_width]
    value_in = row_scale * projected[:, 2 * local_width : 3 * local_width]
    gate_pre = row_scale * projected[:, 3 * local_width : 4 * local_width]
    forget = lower_bound + (1.0 - lower_bound) * jax.nn.sigmoid(forget_pre)
    key_in = 1.0 - forget
    query_act = jax.nn.silu(query_pre)
    head_count = rec_state.shape[1]
    shaped = (seq_count, head_count, HEAD_DIM)
    forget = forget.reshape(shaped)
    key_in = key_in.reshape(shaped)
    value_in = value_in.reshape(shaped)
    query_act = query_act.reshape(shaped)
    new_state = forget[:, :, :, None] * rec_state + key_in[:, :, :, None] * value_in[:, :, None, :]
    head_out = jnp.sum(query_act[:, :, :, None] * new_state, axis=2)
    head_out = head_out * lax.rsqrt(jnp.mean(head_out * head_out, axis=2, keepdims=True) + epsilon)
    head_out = head_out * head_gain.reshape(head_count, HEAD_DIM)
    gated = (head_out.reshape(seq_count, local_width) * jax.nn.silu(gate_pre)).astype(jnp.bfloat16)
    every_head = gather_group(gated, group_count)
    every_head = every_head.reshape(kv_count, tp_count, seq_count, local_width)
    every_head = every_head.transpose(0, 2, 1, 3).reshape(
        kv_count * seq_count, tp_count * local_width
    )
    mixed_add = jnp.dot(every_head, w_heads_out, preferred_element_type=jnp.float32)
    mixed = (tok_float + mixed_add).astype(jnp.bfloat16)
    gathered = gather_group(mixed, group_count).transpose(1, 0, 2).reshape(row_count, model_width)
    terms = channel_mixer(gathered, mixer_gain, w_gate, w_up, w_down)
    out_block = model_width // group_count
    blocked = terms.astype(jnp.bfloat16).reshape(row_count, group_count, out_block)
    blocked = blocked.transpose(1, 0, 2)
    down_sum = jnp.sum(lax.all_to_all(blocked, GROUP, 0, 0).astype(jnp.float32), axis=0)
    result = (mixed.astype(jnp.float32) + down_sum).astype(jnp.bfloat16)
    return (result, new_state)


def solution(mesh):
    placed = (
        P("dp", ("kv", "tp")),
        P(("dp", "kv"), "tp", None, None),
        P(),
        P("kv", "tp"),
        P("kv", "tp"),
        P("kv", "tp"),
        P("kv", "tp"),
        P("tp"),
        P("tp"),
        P(None, ("kv", "tp")),
        P(),
        P(None, ("kv", "tp")),
        P(None, ("kv", "tp")),
        P(("kv", "tp"), None),
    )
    return jax.shard_map(
        local,
        mesh=mesh,
        in_specs=placed,
        out_specs=(P("dp", ("kv", "tp")), P(("dp", "kv"), "tp", None, None)),
        check_vma=False,
    )
```

```python
import jax
import jax.numpy as jnp
from jax import lax
from jax.experimental import pallas as pl
from jax.experimental.pallas import tpu as pltpu
from jax.sharding import PartitionSpec as P

HEAD_DIM = 128
LANES = 128


epsilon = 1e-06
GROUP = ("kv", "tp")
VMEM = pl.BlockSpec(memory_space=pltpu.VMEM)
HBM = pl.BlockSpec(memory_space=pltpu.HBM)


LONG = pl.CostEstimate(flops=10**11, bytes_accessed=10**4, transcendentals=0)
SHORT = pl.CostEstimate(flops=10**7, bytes_accessed=10**4, transcendentals=0)


def resident(array):
    return pltpu.with_memory_space_constraint(array, pltpu.VMEM)


def call(body, outs, *args, streamed=(), scratch=(), limit=6 * 2**20, cost=SHORT):
    return pl.pallas_call(
        body,
        out_shape=outs,
        in_specs=[VMEM] * len(args) + [HBM] * len(streamed),
        out_specs=jax.tree.map(lambda _: VMEM, outs),
        scratch_shapes=scratch,
        compiler_params=pltpu.CompilerParams(vmem_limit_bytes=limit),
        cost_estimate=cost,
    )(*args, *[pltpu.with_memory_space_constraint(w, pltpu.HBM) for w in streamed])


def silu(v):
    return v / (1.0 + jnp.exp(-v))


def project_body(own, other, norm_gain, w_query, w_forget, w_input, w_outgate, out, held, sems):
    copies = [
        pltpu.make_async_copy(weight, held.at[i], sems.at[i])
        for i, weight in enumerate((w_query, w_forget, w_input, w_outgate))
    ]
    for copy in copies:
        copy.start()
    col_block = held.shape[1]
    tp_index = lax.axis_index("tp")
    start = pl.multiple_of(lax.axis_index("kv") * col_block, LANES)
    first = own[...].astype(jnp.float32)
    second = other[...].astype(jnp.float32)
    cols = jnp.concatenate(
        [jnp.where(tp_index == 0, first, second), jnp.where(tp_index == 0, second, first)], axis=1
    )
    squares = jnp.sum(cols * cols, axis=1, keepdims=True)
    scaled = (cols * norm_gain[:, pl.ds(start, col_block)]).astype(jnp.bfloat16)
    spread = jnp.broadcast_to(squares, (squares.shape[0], LANES))
    row = len(copies) * (held.shape[2] // LANES)
    while row < out.shape[1]:
        out[:, row, :] = spread
        row += 1
    row = 0
    for i, copy in enumerate(copies):
        copy.wait()
        product = jnp.dot(scaled, held[i], preferred_element_type=jnp.float32)
        for at in range(0, held.shape[2], LANES):
            out[:, row, :] = product[:, at : at + LANES]
            row += 1


def recur_body(model_width, received, rec_state, lower_bound, head_gain, new_state, gated):
    heads = rec_state.shape[0]
    total = received[0]
    for block in range(1, received.shape[0]):
        total = total + received[block]
    squares = total[4 * heads : 4 * heads + 1, :]
    row_scale = lax.rsqrt(squares / model_width + epsilon)
    query_pre = row_scale * total[:heads]
    forget_pre = row_scale * total[heads : 2 * heads]
    value_in = row_scale * total[2 * heads : 3 * heads]
    gate_pre = row_scale * total[3 * heads : 4 * heads]
    bound = lower_bound[...]
    forget = bound + (1.0 - bound) / (1.0 + jnp.exp(-forget_pre))
    key_in = 1.0 - forget
    query_act = silu(query_pre)
    forget_t = forget.T
    key_t = key_in.T
    query_t = query_act.T
    rows = []
    for h in range(heads):
        fresh = (
            forget_t[:, h : h + 1] * rec_state[h]
            + key_t[:, h : h + 1] * value_in[h : h + 1, :]
        )
        new_state[h] = fresh
        rows.append(jnp.sum(query_t[:, h : h + 1] * fresh, axis=0, keepdims=True))
    head_out = jnp.concatenate(rows, axis=0)
    head_out = head_out * lax.rsqrt(
        jnp.mean(head_out * head_out, axis=1, keepdims=True) + epsilon
    )
    rounded = (head_out * head_gain[...] * silu(gate_pre)).astype(jnp.bfloat16)
    for block in range(gated.shape[0]):
        gated[block] = rounded.astype(jnp.float32)


def heads_body(tp_count, every_head, w_heads_out, tokens, mixed, copies):
    rows, heads = tokens.shape[0], every_head.shape[1]
    left = jnp.concatenate(
        [
            every_head[pl.ds(t, rows, stride=tp_count), h, :]
            for t in range(tp_count)
            for h in range(heads)
        ],
        axis=1,
    ).astype(jnp.bfloat16)
    added = jnp.dot(left, w_heads_out[...], preferred_element_type=jnp.float32)
    rounded = (tokens[...].astype(jnp.float32) + added).astype(jnp.bfloat16)
    mixed[...] = rounded
    for block in range(copies.shape[0]):
        copies[block] = rounded


def mixer_body(gathered, mixer_gain, w_gate, w_up, w_down, out):
    rows = jnp.concatenate([gathered[i] for i in range(gathered.shape[0])], axis=1)
    rows = rows.astype(jnp.float32)
    scale = lax.rsqrt(jnp.mean(rows * rows, axis=1, keepdims=True) + epsilon)
    normed = (rows * scale * mixer_gain[...]).astype(jnp.bfloat16)
    gate_val = jnp.dot(normed, w_gate[...], preferred_element_type=jnp.float32)
    up_val = jnp.dot(normed, w_up[...], preferred_element_type=jnp.float32)
    hidden = (silu(gate_val) * up_val).astype(jnp.bfloat16)
    terms = jnp.dot(hidden, w_down[...], preferred_element_type=jnp.float32)
    terms = terms.astype(jnp.bfloat16)
    width = out.shape[2]
    for i in range(out.shape[0]):
        out[i] = terms[:, i * width : (i + 1) * width]


def result_body(received, mixed, out):
    total = mixed[...].astype(jnp.float32)
    for block in range(received.shape[0]):
        total = total + received[block].astype(jnp.float32)
    out[...] = total.astype(jnp.bfloat16)


def local(
    tokens,
    rec_state,
    norm_gain,
    w_query,
    w_forget,
    w_input,
    w_outgate,
    lower_bound,
    head_gain,
    w_heads_out,
    mixer_gain,
    w_gate,
    w_up,
    w_down,
):
    kv_count = lax.axis_size("kv")
    tp_count = lax.axis_size("tp")
    group_count = kv_count * tp_count
    row_count, own_width = tokens.shape
    heads = rec_state.shape[1]
    model_width = norm_gain.shape[0]
    shape = jax.ShapeDtypeStruct
    other = lax.ppermute(tokens, "tp", [(i, (i + 1) % tp_count) for i in range(tp_count)])
    sent = call(
        project_body,
        shape((row_count, 4 * heads + 8, LANES), jnp.float32),
        tokens,
        other,
        norm_gain[None],
        streamed=(w_query, w_forget, w_input, w_outgate),
        scratch=[
            pltpu.VMEM((4,) + w_query.shape, w_query.dtype),
            pltpu.SemaphoreType.DMA((4,)),
        ],
        limit=12 * 2**20,
        cost=LONG,
    )
    received = lax.all_to_all(sent, "kv", 0, 0)
    new_state, gated = call(
        lambda *refs: recur_body(model_width, *refs),
        (
            shape(rec_state.shape[1:], jnp.float32),
            shape((group_count, heads, HEAD_DIM), jnp.float32),
        ),
        received,
        resident(rec_state[0]),
        lower_bound.reshape(heads, HEAD_DIM),
        head_gain.reshape(heads, HEAD_DIM),
        cost=LONG,
    )
    every_head = lax.all_to_all(gated, GROUP, 0, 0)
    mixed, copies = call(
        lambda *refs: heads_body(tp_count, *refs),
        (
            shape((row_count, own_width), jnp.bfloat16),
            shape((group_count, row_count, own_width), jnp.bfloat16),
        ),
        every_head,
        resident(w_heads_out),
        tokens,
    )
    gathered = lax.all_to_all(copies, GROUP, 0, 0)
    blocked = call(
        mixer_body,
        shape((group_count, row_count, own_width), jnp.bfloat16),
        gathered,
        mixer_gain[None],
        resident(w_gate),
        resident(w_up),
        resident(w_down),
    )
    back = lax.all_to_all(blocked, GROUP, 0, 0)
    result = call(result_body, shape((row_count, own_width), jnp.bfloat16), back, mixed)
    return (result, new_state[None])


def channel_mixer(whole_rows, mixer_gain, w_gate, w_up, w_down):
    rows_float = whole_rows.astype(jnp.float32)
    mixer_scale = lax.rsqrt(jnp.mean(rows_float * rows_float, axis=1, keepdims=True) + epsilon)
    normed = (rows_float * mixer_scale * mixer_gain).astype(jnp.bfloat16)
    gate_val = jnp.dot(normed, w_gate, preferred_element_type=jnp.float32)
    up_val = jnp.dot(normed, w_up, preferred_element_type=jnp.float32)
    hidden = (jax.nn.silu(gate_val) * up_val).astype(jnp.bfloat16)
    return jnp.dot(hidden, w_down, preferred_element_type=jnp.float32)


def gather_group(block, count):
    copies = jnp.broadcast_to(block[None], (count,) + block.shape)
    return lax.all_to_all(copies, GROUP, 0, 0)


def plain_local(
    tokens,
    rec_state,
    norm_gain,
    w_query,
    w_forget,
    w_input,
    w_outgate,
    lower_bound,
    head_gain,
    w_heads_out,
    mixer_gain,
    w_gate,
    w_up,
    w_down,
):
    kv_count = lax.axis_size("kv")
    tp_count = lax.axis_size("tp")
    kv_index = lax.axis_index("kv")
    tp_index = lax.axis_index("tp")
    group_count = kv_count * tp_count
    row_count = tokens.shape[0]
    seq_count = rec_state.shape[0]
    model_width = norm_gain.shape[0]
    col_block = model_width // kv_count
    tok_float = tokens.astype(jnp.float32)
    other = lax.ppermute(tokens, "tp", [(i, (i + 1) % tp_count) for i in range(tp_count)])
    low = jnp.where(tp_index == 0, tokens, other)
    high = jnp.where(tp_index == 0, other, tokens)
    own_cols = jnp.concatenate([low, high], axis=1).astype(jnp.float32)
    squares = jnp.sum(own_cols * own_cols, axis=1)
    gain_block = lax.dynamic_slice_in_dim(norm_gain, kv_index * col_block, col_block, 0)
    scaled = (own_cols * gain_block).astype(jnp.bfloat16)
    partial = [
        jnp.dot(scaled, weight, preferred_element_type=jnp.float32)
        for weight in (w_query, w_forget, w_input, w_outgate)
    ]
    local_width = w_query.shape[1]
    partial.append(jnp.broadcast_to(squares[:, None], (row_count, 128)))
    sent = jnp.concatenate(partial, axis=1).reshape(kv_count, seq_count, -1)
    projected = jnp.sum(lax.all_to_all(sent, "kv", 0, 0), axis=0)
    my_squares = projected[:, 4 * local_width]
    row_scale = lax.rsqrt(my_squares / model_width + epsilon)[:, None]
    query_pre = row_scale * projected[:, :local_width]
    forget_pre = row_scale * projected[:, local_width : 2 * local_width]
    value_in = row_scale * projected[:, 2 * local_width : 3 * local_width]
    gate_pre = row_scale * projected[:, 3 * local_width : 4 * local_width]
    forget = lower_bound + (1.0 - lower_bound) * jax.nn.sigmoid(forget_pre)
    key_in = 1.0 - forget
    query_act = jax.nn.silu(query_pre)
    head_count = rec_state.shape[1]
    shaped = (seq_count, head_count, HEAD_DIM)
    forget = forget.reshape(shaped)
    key_in = key_in.reshape(shaped)
    value_in = value_in.reshape(shaped)
    query_act = query_act.reshape(shaped)
    new_state = forget[:, :, :, None] * rec_state + key_in[:, :, :, None] * value_in[:, :, None, :]
    head_out = jnp.sum(query_act[:, :, :, None] * new_state, axis=2)
    head_out = head_out * lax.rsqrt(jnp.mean(head_out * head_out, axis=2, keepdims=True) + epsilon)
    head_out = head_out * head_gain.reshape(head_count, HEAD_DIM)
    gated = (head_out.reshape(seq_count, local_width) * jax.nn.silu(gate_pre)).astype(jnp.bfloat16)
    every_head = gather_group(gated, group_count)
    every_head = every_head.reshape(kv_count, tp_count, seq_count, local_width)
    every_head = every_head.transpose(0, 2, 1, 3).reshape(
        kv_count * seq_count, tp_count * local_width
    )
    mixed_add = jnp.dot(every_head, w_heads_out, preferred_element_type=jnp.float32)
    mixed = (tok_float + mixed_add).astype(jnp.bfloat16)
    gathered = gather_group(mixed, group_count).transpose(1, 0, 2).reshape(row_count, model_width)
    terms = channel_mixer(gathered, mixer_gain, w_gate, w_up, w_down)
    out_block = model_width // group_count
    blocked = terms.astype(jnp.bfloat16).reshape(row_count, group_count, out_block)
    blocked = blocked.transpose(1, 0, 2)
    down_sum = jnp.sum(lax.all_to_all(blocked, GROUP, 0, 0).astype(jnp.float32), axis=0)
    result = (mixed.astype(jnp.float32) + down_sum).astype(jnp.bfloat16)
    return (result, new_state)


def choose(*args):
    tokens, rec_state = args[0], args[1]
    w_heads_out, w_gate = args[9], args[11]
    aligned = all(size % LANES == 0 for size in (tokens.shape[1], w_gate.shape[1]))
    if aligned and rec_state.shape[0] == 1 and lax.axis_size("tp") == 2:
        return local(*args)
    return plain_local(*args)


def solution(mesh):
    placed = (
        P("dp", ("kv", "tp")),
        P(("dp", "kv"), "tp", None, None),
        P(),
        P("kv", "tp"),
        P("kv", "tp"),
        P("kv", "tp"),
        P("kv", "tp"),
        P("tp"),
        P("tp"),
        P(None, ("kv", "tp")),
        P(),
        P(None, ("kv", "tp")),
        P(None, ("kv", "tp")),
        P(("kv", "tp"), None),
    )
    return jax.shard_map(
        choose,
        mesh=mesh,
        in_specs=placed,
        out_specs=(P("dp", ("kv", "tp")), P(("dp", "kv"), "tp", None, None)),
        check_vma=False,
    )
```

```python
import jax
import jax.numpy as jnp
from jax import lax
from jax.experimental import pallas as pl
from jax.experimental.pallas import tpu as pltpu
from jax.sharding import PartitionSpec as P

HEAD_DIM = 128
LANES = 128


epsilon = 1e-06
GROUP = ("kv", "tp")
VMEM = pl.BlockSpec(memory_space=pltpu.VMEM)
HBM = pl.BlockSpec(memory_space=pltpu.HBM)


LONG = pl.CostEstimate(flops=10**11, bytes_accessed=10**4, transcendentals=0)
SHORT = pl.CostEstimate(flops=10**7, bytes_accessed=10**4, transcendentals=0)


def resident(array):
    return pltpu.with_memory_space_constraint(array, pltpu.VMEM)


def call(body, outs, *args, streamed=(), scratch=(), limit=6 * 2**20, cost=SHORT):
    return pl.pallas_call(
        body,
        out_shape=outs,
        in_specs=[VMEM] * len(args) + [HBM] * len(streamed),
        out_specs=jax.tree.map(lambda _: VMEM, outs),
        scratch_shapes=scratch,
        compiler_params=pltpu.CompilerParams(vmem_limit_bytes=limit),
        cost_estimate=cost,
    )(*args, *[pltpu.with_memory_space_constraint(w, pltpu.HBM) for w in streamed])


def silu(v):
    return v / (1.0 + jnp.exp(-v))


def start_body(
    tokens, norm_gain, w_query, w_forget, w_input, w_outgate,
    own, squares, other_gain, rest, held, held_tokens, held_gain, sems,
):
    half = held.shape[1]
    tp_index, base = lax.axis_index("tp"), lax.axis_index("kv") * 2 * half
    mine = pl.multiple_of(tp_index * half, LANES)
    theirs = pl.multiple_of((1 - tp_index) * half, LANES)
    weights = (w_query, w_forget, w_input, w_outgate)
    moves = [
        (tokens, held_tokens),
        (norm_gain.at[:, pl.ds(pl.multiple_of(base + mine, LANES), half)], held_gain),
        *[(w.at[pl.ds(mine, half), :], held.at[i]) for i, w in enumerate(weights)],
        (norm_gain.at[:, pl.ds(pl.multiple_of(base + theirs, LANES), half)], other_gain),
        *[(w.at[pl.ds(theirs, half), :], rest.at[i]) for i, w in enumerate(weights)],
    ]
    copies = [pltpu.make_async_copy(src, dst, sems.at[i]) for i, (src, dst) in enumerate(moves)]
    for copy in copies:
        copy.start()
    copies[0].wait()
    copies[1].wait()
    cols = held_tokens[...].astype(jnp.float32)
    squares[...] = jnp.broadcast_to(
        jnp.sum(cols * cols, axis=1, keepdims=True), (cols.shape[0], LANES)
    )
    scaled = (cols * held_gain[...]).astype(jnp.bfloat16)
    for i in range(len(weights)):
        copies[2 + i].wait()
        own[i] = jnp.dot(scaled, held[i], preferred_element_type=jnp.float32)
    for copy in copies[2 + len(weights) :]:
        copy.wait()


def project_body(other, own, own_squares, other_gain, rest, kept, *sent_and_scratch):
    *sent, every = sent_and_scratch
    kv_index = lax.axis_index("kv")
    cols = other[...].astype(jnp.float32)
    squares = own_squares[...] + jnp.sum(cols * cols, axis=1, keepdims=True)
    scaled = (cols * other_gain[...]).astype(jnp.bfloat16)
    row = 0
    for i in range(rest.shape[0]):
        product = own[i] + jnp.dot(scaled, rest[i], preferred_element_type=jnp.float32)
        for at in range(0, product.shape[1], LANES):
            every[:, row, :] = product[:, at : at + LANES]
            row += 1
    for at in range(row, every.shape[1]):
        every[:, at, :] = squares
    kept[...] = every[kv_index]
    for j, out in enumerate(sent, 1):
        block = every[kv_index ^ j]
        high = block[row:].astype(jnp.bfloat16).astype(jnp.float32)
        wide = jnp.concatenate([block[:row], high, block[row:] - high], axis=0)
        out[...] = wide.astype(jnp.bfloat16)


def recur_body(model_width, arrived, *refs):
    kept, *received = refs[: arrived + 1]
    rec_state, lower_bound, head_gain, new_state, gated = refs[arrived + 1 :]
    heads = rec_state.shape[0]
    row = 4 * heads
    total = kept[:row]
    squares = kept[row : row + 8]
    for block in received:
        wide = block[...].astype(jnp.float32)
        total = total + wide[:row]
        squares = squares + wide[row : row + 8] + wide[row + 8 : row + 16]
    row_scale = lax.rsqrt(squares[:1] / model_width + epsilon)
    query_pre = row_scale * total[:heads]
    forget_pre = row_scale * total[heads : 2 * heads]
    value_in = row_scale * total[2 * heads : 3 * heads]
    gate_pre = row_scale * total[3 * heads : 4 * heads]
    bound = lower_bound[...]
    forget = bound + (1.0 - bound) / (1.0 + jnp.exp(-forget_pre))
    key_in = 1.0 - forget
    query_act = silu(query_pre)
    forget_t = forget.T
    key_t = key_in.T
    query_t = query_act.T
    rows = []
    for h in range(heads):
        fresh = (
            forget_t[:, h : h + 1] * rec_state[h]
            + key_t[:, h : h + 1] * value_in[h : h + 1, :]
        )
        new_state[h] = fresh
        rows.append(jnp.sum(query_t[:, h : h + 1] * fresh, axis=0, keepdims=True))
    head_out = jnp.concatenate(rows, axis=0)
    head_out = head_out * lax.rsqrt(
        jnp.mean(head_out * head_out, axis=1, keepdims=True) + epsilon
    )
    rounded = (head_out * head_gain[...] * silu(gate_pre)).astype(jnp.bfloat16)
    for block in range(gated.shape[0]):
        gated[block] = rounded.astype(jnp.float32)


def heads_body(tp_count, every_head, w_heads_out, tokens, mixed, copies):
    rows, heads = tokens.shape[0], every_head.shape[1]
    left = jnp.concatenate(
        [
            every_head[pl.ds(t, rows, stride=tp_count), h, :]
            for t in range(tp_count)
            for h in range(heads)
        ],
        axis=1,
    ).astype(jnp.bfloat16)
    added = jnp.dot(left, w_heads_out[...], preferred_element_type=jnp.float32)
    rounded = (tokens[...].astype(jnp.float32) + added).astype(jnp.bfloat16)
    mixed[...] = rounded
    for block in range(copies.shape[0]):
        copies[block] = rounded


def mixer_body(gathered, mixer_gain, w_gate, w_up, w_down, out):
    rows = jnp.concatenate([gathered[i] for i in range(gathered.shape[0])], axis=1)
    rows = rows.astype(jnp.float32)
    scale = lax.rsqrt(jnp.mean(rows * rows, axis=1, keepdims=True) + epsilon)
    normed = (rows * scale * mixer_gain[...]).astype(jnp.bfloat16)
    gate_val = jnp.dot(normed, w_gate[...], preferred_element_type=jnp.float32)
    up_val = jnp.dot(normed, w_up[...], preferred_element_type=jnp.float32)
    hidden = (silu(gate_val) * up_val).astype(jnp.bfloat16)
    terms = jnp.dot(hidden, w_down[...], preferred_element_type=jnp.float32)
    terms = terms.astype(jnp.bfloat16)
    width = out.shape[2]
    for i in range(out.shape[0]):
        out[i] = terms[:, i * width : (i + 1) * width]


def result_body(received, mixed, out):
    total = mixed[...].astype(jnp.float32)
    for block in range(received.shape[0]):
        total = total + received[block].astype(jnp.float32)
    out[...] = total.astype(jnp.bfloat16)


def local(
    tokens,
    rec_state,
    norm_gain,
    w_query,
    w_forget,
    w_input,
    w_outgate,
    lower_bound,
    head_gain,
    w_heads_out,
    mixer_gain,
    w_gate,
    w_up,
    w_down,
):
    kv_count = lax.axis_size("kv")
    tp_count = lax.axis_size("tp")
    group_count = kv_count * tp_count
    row_count, own_width = tokens.shape
    heads = rec_state.shape[1]
    model_width = norm_gain.shape[0]
    shape = jax.ShapeDtypeStruct
    other = lax.ppermute(tokens, "tp", [(i, (i + 1) % tp_count) for i in range(tp_count)])
    weights = (w_query, w_forget, w_input, w_outgate)
    half_shape = (4, own_width, w_query.shape[1])
    own, squares, other_gain, rest = call(
        start_body,
        (
            shape((4, row_count, w_query.shape[1]), jnp.float32),
            shape((row_count, LANES), jnp.float32),
            pltpu.VMEM((1, own_width), jnp.float32),
            pltpu.VMEM(half_shape, w_query.dtype),
        ),
        streamed=(tokens, norm_gain[None], *weights),
        scratch=[
            pltpu.VMEM(half_shape, w_query.dtype),
            pltpu.VMEM(tokens.shape, tokens.dtype),
            pltpu.VMEM((1, own_width), jnp.float32),
            pltpu.SemaphoreType.DMA((3 + 2 * len(weights),)),
        ],
        limit=12 * 2**20,
    )
    rows = 4 * heads
    kept, *sent = call(
        project_body,
        (
            shape((rows + 8, LANES), jnp.float32),
            *[shape((rows + 16, LANES), jnp.bfloat16)] * (kv_count - 1),
        ),
        other,
        own,
        squares,
        resident(other_gain),
        resident(rest),
        scratch=[pltpu.VMEM((row_count, rows + 8, LANES), jnp.float32)],
        cost=LONG,
    )
    received = [
        lax.ppermute(block, "kv", [(i, i ^ j) for i in range(kv_count)])
        for j, block in enumerate(sent, 1)
    ]
    new_state, gated = call(
        lambda *refs: recur_body(model_width, len(received), *refs),
        (
            pltpu.VMEM(rec_state.shape[1:], jnp.float32),
            shape((group_count, heads, HEAD_DIM), jnp.float32),
        ),
        kept,
        *received,
        resident(rec_state[0]),
        lower_bound.reshape(heads, HEAD_DIM),
        head_gain.reshape(heads, HEAD_DIM),
        cost=LONG,
    )
    every_head = lax.all_to_all(gated, GROUP, 0, 0)
    mixed, copies = call(
        lambda *refs: heads_body(tp_count, *refs),
        (
            shape((row_count, own_width), jnp.bfloat16),
            shape((group_count, row_count, own_width), jnp.bfloat16),
        ),
        every_head,
        resident(w_heads_out),
        tokens,
    )
    gathered = lax.all_to_all(copies, GROUP, 0, 0)
    blocked = call(
        mixer_body,
        shape((group_count, row_count, own_width), jnp.bfloat16),
        gathered,
        mixer_gain[None],
        resident(w_gate),
        resident(w_up),
        resident(w_down),
    )
    back = lax.all_to_all(blocked, GROUP, 0, 0)
    result = call(result_body, shape((row_count, own_width), jnp.bfloat16), back, mixed)
    return (result, new_state[None])


def channel_mixer(whole_rows, mixer_gain, w_gate, w_up, w_down):
    rows_float = whole_rows.astype(jnp.float32)
    mixer_scale = lax.rsqrt(jnp.mean(rows_float * rows_float, axis=1, keepdims=True) + epsilon)
    normed = (rows_float * mixer_scale * mixer_gain).astype(jnp.bfloat16)
    gate_val = jnp.dot(normed, w_gate, preferred_element_type=jnp.float32)
    up_val = jnp.dot(normed, w_up, preferred_element_type=jnp.float32)
    hidden = (jax.nn.silu(gate_val) * up_val).astype(jnp.bfloat16)
    return jnp.dot(hidden, w_down, preferred_element_type=jnp.float32)


def gather_group(block, count):
    copies = jnp.broadcast_to(block[None], (count,) + block.shape)
    return lax.all_to_all(copies, GROUP, 0, 0)


def plain_local(
    tokens,
    rec_state,
    norm_gain,
    w_query,
    w_forget,
    w_input,
    w_outgate,
    lower_bound,
    head_gain,
    w_heads_out,
    mixer_gain,
    w_gate,
    w_up,
    w_down,
):
    kv_count = lax.axis_size("kv")
    tp_count = lax.axis_size("tp")
    kv_index = lax.axis_index("kv")
    tp_index = lax.axis_index("tp")
    group_count = kv_count * tp_count
    row_count = tokens.shape[0]
    seq_count = rec_state.shape[0]
    model_width = norm_gain.shape[0]
    col_block = model_width // kv_count
    tok_float = tokens.astype(jnp.float32)
    other = lax.ppermute(tokens, "tp", [(i, (i + 1) % tp_count) for i in range(tp_count)])
    low = jnp.where(tp_index == 0, tokens, other)
    high = jnp.where(tp_index == 0, other, tokens)
    own_cols = jnp.concatenate([low, high], axis=1).astype(jnp.float32)
    squares = jnp.sum(own_cols * own_cols, axis=1)
    gain_block = lax.dynamic_slice_in_dim(norm_gain, kv_index * col_block, col_block, 0)
    scaled = (own_cols * gain_block).astype(jnp.bfloat16)
    partial = [
        jnp.dot(scaled, weight, preferred_element_type=jnp.float32)
        for weight in (w_query, w_forget, w_input, w_outgate)
    ]
    local_width = w_query.shape[1]
    partial.append(jnp.broadcast_to(squares[:, None], (row_count, 128)))
    sent = jnp.concatenate(partial, axis=1).reshape(kv_count, seq_count, -1)
    projected = jnp.sum(lax.all_to_all(sent, "kv", 0, 0), axis=0)
    my_squares = projected[:, 4 * local_width]
    row_scale = lax.rsqrt(my_squares / model_width + epsilon)[:, None]
    query_pre = row_scale * projected[:, :local_width]
    forget_pre = row_scale * projected[:, local_width : 2 * local_width]
    value_in = row_scale * projected[:, 2 * local_width : 3 * local_width]
    gate_pre = row_scale * projected[:, 3 * local_width : 4 * local_width]
    forget = lower_bound + (1.0 - lower_bound) * jax.nn.sigmoid(forget_pre)
    key_in = 1.0 - forget
    query_act = jax.nn.silu(query_pre)
    head_count = rec_state.shape[1]
    shaped = (seq_count, head_count, HEAD_DIM)
    forget = forget.reshape(shaped)
    key_in = key_in.reshape(shaped)
    value_in = value_in.reshape(shaped)
    query_act = query_act.reshape(shaped)
    new_state = forget[:, :, :, None] * rec_state + key_in[:, :, :, None] * value_in[:, :, None, :]
    head_out = jnp.sum(query_act[:, :, :, None] * new_state, axis=2)
    head_out = head_out * lax.rsqrt(jnp.mean(head_out * head_out, axis=2, keepdims=True) + epsilon)
    head_out = head_out * head_gain.reshape(head_count, HEAD_DIM)
    gated = (head_out.reshape(seq_count, local_width) * jax.nn.silu(gate_pre)).astype(jnp.bfloat16)
    every_head = gather_group(gated, group_count)
    every_head = every_head.reshape(kv_count, tp_count, seq_count, local_width)
    every_head = every_head.transpose(0, 2, 1, 3).reshape(
        kv_count * seq_count, tp_count * local_width
    )
    mixed_add = jnp.dot(every_head, w_heads_out, preferred_element_type=jnp.float32)
    mixed = (tok_float + mixed_add).astype(jnp.bfloat16)
    gathered = gather_group(mixed, group_count).transpose(1, 0, 2).reshape(row_count, model_width)
    terms = channel_mixer(gathered, mixer_gain, w_gate, w_up, w_down)
    out_block = model_width // group_count
    blocked = terms.astype(jnp.bfloat16).reshape(row_count, group_count, out_block)
    blocked = blocked.transpose(1, 0, 2)
    down_sum = jnp.sum(lax.all_to_all(blocked, GROUP, 0, 0).astype(jnp.float32), axis=0)
    result = (mixed.astype(jnp.float32) + down_sum).astype(jnp.bfloat16)
    return (result, new_state)


def choose(*args):
    tokens, rec_state = args[0], args[1]
    w_heads_out, w_gate = args[9], args[11]
    aligned = all(size % LANES == 0 for size in (tokens.shape[1], w_gate.shape[1]))
    small = lax.axis_size("tp") == 2 and lax.axis_size("kv") in (2, 4)
    if aligned and small and rec_state.shape[0] == 1:
        return local(*args)
    return plain_local(*args)


def solution(mesh):
    placed = (
        P("dp", ("kv", "tp")),
        P(("dp", "kv"), "tp", None, None),
        P(),
        P("kv", "tp"),
        P("kv", "tp"),
        P("kv", "tp"),
        P("kv", "tp"),
        P("tp"),
        P("tp"),
        P(None, ("kv", "tp")),
        P(),
        P(None, ("kv", "tp")),
        P(None, ("kv", "tp")),
        P(("kv", "tp"), None),
    )
    return jax.shard_map(
        choose,
        mesh=mesh,
        in_specs=placed,
        out_specs=(P("dp", ("kv", "tp")), P(("dp", "kv"), "tp", None, None)),
        check_vma=False,
    )
```

```python
import jax
import jax.numpy as jnp
from jax import lax
from jax.experimental import pallas as pl
from jax.experimental.pallas import tpu as pltpu
from jax.sharding import PartitionSpec as P

HEAD_DIM = 128
LANES = 128


epsilon = 1e-06
GROUP = ("kv", "tp")
VMEM = pl.BlockSpec(memory_space=pltpu.VMEM)
HBM = pl.BlockSpec(memory_space=pltpu.HBM)


LONG = pl.CostEstimate(flops=10**11, bytes_accessed=10**4, transcendentals=0)
SHORT = pl.CostEstimate(flops=10**7, bytes_accessed=10**4, transcendentals=0)


def resident(array):
    return pltpu.with_memory_space_constraint(array, pltpu.VMEM)


def call(body, outs, *args, streamed=(), scratch=(), limit=6 * 2**20, cost=SHORT):
    return pl.pallas_call(
        body,
        out_shape=outs,
        in_specs=[VMEM] * len(args) + [HBM] * len(streamed),
        out_specs=jax.tree.map(lambda _: VMEM, outs),
        scratch_shapes=scratch,
        compiler_params=pltpu.CompilerParams(vmem_limit_bytes=limit),
        cost_estimate=cost,
    )(*args, *[pltpu.with_memory_space_constraint(w, pltpu.HBM) for w in streamed])


def silu(v):
    return v / (1.0 + jnp.exp(-v))


def start_body(
    tokens, norm_gain, w_query, w_forget, w_input, w_outgate,
    own, squares, other_gain, rest, held, held_tokens, held_gain, sems,
):
    half = held.shape[1]
    tp_index, base = lax.axis_index("tp"), lax.axis_index("kv") * 2 * half
    mine = pl.multiple_of(tp_index * half, LANES)
    theirs = pl.multiple_of((1 - tp_index) * half, LANES)
    weights = (w_query, w_forget, w_input, w_outgate)
    moves = [
        (tokens, held_tokens),
        (norm_gain.at[:, pl.ds(pl.multiple_of(base + mine, LANES), half)], held_gain),
        *[(w.at[pl.ds(mine, half), :], held.at[i]) for i, w in enumerate(weights)],
        (norm_gain.at[:, pl.ds(pl.multiple_of(base + theirs, LANES), half)], other_gain),
        *[(w.at[pl.ds(theirs, half), :], rest.at[i]) for i, w in enumerate(weights)],
    ]
    copies = [pltpu.make_async_copy(src, dst, sems.at[i]) for i, (src, dst) in enumerate(moves)]
    for copy in copies:
        copy.start()
    copies[0].wait()
    copies[1].wait()
    cols = held_tokens[...].astype(jnp.float32)
    squares[...] = jnp.broadcast_to(
        jnp.sum(cols * cols, axis=1, keepdims=True), (cols.shape[0], LANES)
    )
    scaled = (cols * held_gain[...]).astype(jnp.bfloat16)
    for i in range(len(weights)):
        copies[2 + i].wait()
        own[i] = jnp.dot(scaled, held[i], preferred_element_type=jnp.float32)
    for copy in copies[2 + len(weights) :]:
        copy.wait()


def project_body(other, own, own_squares, other_gain, rest, kept, *sent_and_scratch):
    *sent, every = sent_and_scratch
    kv_index = lax.axis_index("kv")
    cols = other[...].astype(jnp.float32)
    squares = own_squares[...] + jnp.sum(cols * cols, axis=1, keepdims=True)
    scaled = (cols * other_gain[...]).astype(jnp.bfloat16)
    row = 0
    for i in range(rest.shape[0]):
        product = own[i] + jnp.dot(scaled, rest[i], preferred_element_type=jnp.float32)
        for at in range(0, product.shape[1], LANES):
            every[:, row, :] = product[:, at : at + LANES]
            row += 1
    for at in range(row, every.shape[1]):
        every[:, at, :] = squares
    kept[...] = every[kv_index]
    for j, out in enumerate(sent, 1):
        block = every[kv_index ^ j]
        high = block[row:].astype(jnp.bfloat16).astype(jnp.float32)
        wide = jnp.concatenate([block[:row], high, block[row:] - high], axis=0)
        out[...] = wide.astype(jnp.bfloat16)


def recur_body(model_width, arrived, *refs):
    kept, *received = refs[: arrived + 1]
    rec_state, lower_bound, head_gain, new_state, gated = refs[arrived + 1 :]
    heads = rec_state.shape[0]
    row = 4 * heads
    total = kept[:row]
    squares = kept[row : row + 8]
    for block in received:
        wide = block[...].astype(jnp.float32)
        total = total + wide[:row]
        squares = squares + wide[row : row + 8] + wide[row + 8 : row + 16]
    row_scale = lax.rsqrt(squares[:1] / model_width + epsilon)
    query_pre = row_scale * total[:heads]
    forget_pre = row_scale * total[heads : 2 * heads]
    value_in = row_scale * total[2 * heads : 3 * heads]
    gate_pre = row_scale * total[3 * heads : 4 * heads]
    bound = lower_bound[...]
    forget = bound + (1.0 - bound) / (1.0 + jnp.exp(-forget_pre))
    key_in = 1.0 - forget
    query_act = silu(query_pre)
    forget_t = forget.T
    key_t = key_in.T
    query_t = query_act.T
    rows = []
    for h in range(heads):
        fresh = (
            forget_t[:, h : h + 1] * rec_state[h]
            + key_t[:, h : h + 1] * value_in[h : h + 1, :]
        )
        new_state[h] = fresh
        rows.append(jnp.sum(query_t[:, h : h + 1] * fresh, axis=0, keepdims=True))
    head_out = jnp.concatenate(rows, axis=0)
    head_out = head_out * lax.rsqrt(
        jnp.mean(head_out * head_out, axis=1, keepdims=True) + epsilon
    )
    rounded = (head_out * head_gain[...] * silu(gate_pre)).astype(jnp.bfloat16)
    gated[...] = rounded.astype(jnp.float32)


def pair_body(own, other, out):
    first = lax.axis_index("tp") == 0
    left = own[...].astype(jnp.float32)
    right = other[...].astype(jnp.float32)
    low, high = jnp.where(first, left, right), jnp.where(first, right, left)
    out[...] = jnp.concatenate([low, high], axis=0).astype(out.dtype).reshape(out.shape)


def heads_body(*refs):
    *blocks, w_heads_out, tokens, mixed, every = refs
    kv_index = lax.axis_index("kv")
    for j, block in enumerate(blocks):
        every[kv_index ^ j] = block[...].astype(jnp.float32)
    left = jnp.concatenate([every[:, h, :] for h in range(every.shape[1])], axis=1)
    added = jnp.dot(
        left.astype(jnp.bfloat16), w_heads_out[...], preferred_element_type=jnp.float32
    )
    mixed[...] = (tokens[...].astype(jnp.float32) + added).astype(jnp.bfloat16)


def mixer_block(j, block, mixer_gain, w_gate, w_up):
    depth = block.shape[0] * block.shape[2]
    start = pl.multiple_of((lax.axis_index("kv") ^ j) * depth, LANES)
    cols = jnp.concatenate([block[t] for t in range(block.shape[0])], axis=1)
    cols = cols.astype(jnp.float32)
    squares = jnp.sum(cols * cols, axis=1, keepdims=True)
    gained = (cols * mixer_gain[:, pl.ds(start, depth)]).astype(jnp.bfloat16)
    return (
        jnp.dot(gained, w_gate[pl.ds(start, depth), :], preferred_element_type=jnp.float32),
        jnp.dot(gained, w_up[pl.ds(start, depth), :], preferred_element_type=jnp.float32),
        squares,
    )


def mixer_own_body(block, mixer_gain, w_gate, w_up, w_down, gate, up, squares):
    gate[...], up[...], summed = mixer_block(0, block, mixer_gain, w_gate, w_up)
    squares[...] = jnp.broadcast_to(summed, squares.shape)


def down_block(hidden, w_down, chip, core, width):
    start = pl.multiple_of((chip * 2 + core) * width, LANES)
    return jnp.dot(hidden, w_down[:, pl.ds(start, width)], preferred_element_type=jnp.float32)


def mixer_body(*refs):
    gate, up, squares, *blocks = refs[:-6]
    mixer_gain, w_gate, w_up, w_down, hidden, passed = refs[-6:]
    gate_val, up_val, total = gate[...], up[...], squares[:, :1]
    for j, block in enumerate(blocks, 1):
        more_gate, more_up, more = mixer_block(j, block, mixer_gain, w_gate, w_up)
        gate_val, up_val, total = gate_val + more_gate, up_val + more_up, total + more
    scale = lax.rsqrt(total / w_gate.shape[0] + epsilon)
    gate_val, up_val = scale * gate_val, scale * up_val
    active = (silu(gate_val) * up_val).astype(jnp.bfloat16)
    hidden[...] = active
    kv_index, tp_index = lax.axis_index("kv"), lax.axis_index("tp")
    for j in range(passed.shape[0]):
        core = 1 - tp_index if j == 0 else tp_index
        passed[j] = down_block(active, w_down, kv_index ^ j, core, passed.shape[2]).astype(
            jnp.bfloat16
        )


def down_body(hidden, w_down, sums):
    kv_index, tp_index = lax.axis_index("kv"), lax.axis_index("tp")
    for j in range(sums.shape[0]):
        core = tp_index if j == 0 else 1 - tp_index
        sums[j] = down_block(hidden[...], w_down, kv_index ^ j, core, sums.shape[2])


def chip_sum_body(sums, passed, mixed, base, *sent):
    base[...] = mixed[...].astype(jnp.float32) + sums[0] + passed[0].astype(jnp.float32)
    for j, out in enumerate(sent, 1):
        out[...] = (sums[j] + passed[j].astype(jnp.float32)).astype(jnp.bfloat16)


def result_body(base, *refs):
    *received, out = refs
    total = base[...]
    for block in received:
        total = total + block[...].astype(jnp.float32)
    out[...] = total.astype(jnp.bfloat16)


def local(
    tokens,
    rec_state,
    norm_gain,
    w_query,
    w_forget,
    w_input,
    w_outgate,
    lower_bound,
    head_gain,
    w_heads_out,
    mixer_gain,
    w_gate,
    w_up,
    w_down,
):
    kv_count = lax.axis_size("kv")
    tp_count = lax.axis_size("tp")
    group_count = kv_count * tp_count
    row_count, own_width = tokens.shape
    heads = rec_state.shape[1]
    model_width = norm_gain.shape[0]
    shape = jax.ShapeDtypeStruct
    other = lax.ppermute(tokens, "tp", [(i, (i + 1) % tp_count) for i in range(tp_count)])
    weights = (w_query, w_forget, w_input, w_outgate)
    half_shape = (4, own_width, w_query.shape[1])
    own, squares, other_gain, rest = call(
        start_body,
        (
            shape((4, row_count, w_query.shape[1]), jnp.float32),
            shape((row_count, LANES), jnp.float32),
            pltpu.VMEM((1, own_width), jnp.float32),
            pltpu.VMEM(half_shape, w_query.dtype),
        ),
        streamed=(tokens, norm_gain[None], *weights),
        scratch=[
            pltpu.VMEM(half_shape, w_query.dtype),
            pltpu.VMEM(tokens.shape, tokens.dtype),
            pltpu.VMEM((1, own_width), jnp.float32),
            pltpu.SemaphoreType.DMA((3 + 2 * len(weights),)),
        ],
        limit=12 * 2**20,
    )
    rows = 4 * heads
    kept, *sent = call(
        project_body,
        (
            shape((rows + 8, LANES), jnp.float32),
            *[shape((rows + 16, LANES), jnp.bfloat16)] * (kv_count - 1),
        ),
        other,
        own,
        squares,
        resident(other_gain),
        resident(rest),
        scratch=[pltpu.VMEM((row_count, rows + 8, LANES), jnp.float32)],
        cost=LONG,
    )
    received = [
        lax.ppermute(block, "kv", [(i, i ^ j) for i in range(kv_count)])
        for j, block in enumerate(sent, 1)
    ]
    new_state, gated = call(
        lambda *refs: recur_body(model_width, len(received), *refs),
        (
            pltpu.VMEM(rec_state.shape[1:], jnp.float32),
            shape((heads, HEAD_DIM), jnp.float32),
        ),
        kept,
        *received,
        resident(rec_state[0]),
        lower_bound.reshape(heads, HEAD_DIM),
        head_gain.reshape(heads, HEAD_DIM),
        cost=LONG,
    )

    def swapped(block):
        return lax.ppermute(block, "tp", [(0, 1), (1, 0)])

    def crossed(block, j):
        return lax.ppermute(block, GROUP, [(i, i ^ (2 * j + 1)) for i in range(group_count)])

    others = range(1, kv_count)
    pair = call(
        pair_body, shape((2 * heads, HEAD_DIM), jnp.bfloat16), gated, swapped(gated)
    )
    mixed = call(
        heads_body,
        shape((row_count, own_width), jnp.bfloat16),
        pair,
        *[crossed(pair, j) for j in others],
        resident(w_heads_out),
        tokens,
        scratch=[pltpu.VMEM((kv_count, 2 * heads, HEAD_DIM), jnp.float32)],
    )
    pair = call(
        pair_body, shape((2, row_count, own_width), jnp.bfloat16), mixed, swapped(mixed)
    )
    blocks = [crossed(pair, j) for j in others]
    gain = mixer_gain[None]
    w_gate, w_up, w_down = resident(w_gate), resident(w_up), resident(w_down)
    width = w_gate.shape[1]
    products = call(
        mixer_own_body,
        (
            shape((row_count, width), jnp.float32),
            shape((row_count, width), jnp.float32),
            shape((row_count, LANES), jnp.float32),
        ),
        pair,
        gain,
        w_gate,
        w_up,
        w_down,
    )
    hidden, passed = call(
        mixer_body,
        (
            shape((row_count, width), jnp.bfloat16),
            shape((kv_count, row_count, own_width), jnp.bfloat16),
        ),
        *products,
        *blocks,
        gain,
        w_gate,
        w_up,
        w_down,
    )
    passed = swapped(passed)
    sums = call(down_body, shape(passed.shape, jnp.float32), hidden, w_down)
    base, *sent = call(
        chip_sum_body,
        (
            shape(mixed.shape, jnp.float32),
            *[shape(mixed.shape, jnp.bfloat16)] * (kv_count - 1),
        ),
        sums,
        passed,
        mixed,
    )
    result = call(
        result_body,
        shape(mixed.shape, jnp.bfloat16),
        base,
        *[crossed(block, j) for j, block in enumerate(sent, 1)],
    )
    return (result, new_state[None])


def channel_mixer(whole_rows, mixer_gain, w_gate, w_up, w_down):
    rows_float = whole_rows.astype(jnp.float32)
    mixer_scale = lax.rsqrt(jnp.mean(rows_float * rows_float, axis=1, keepdims=True) + epsilon)
    normed = (rows_float * mixer_scale * mixer_gain).astype(jnp.bfloat16)
    gate_val = jnp.dot(normed, w_gate, preferred_element_type=jnp.float32)
    up_val = jnp.dot(normed, w_up, preferred_element_type=jnp.float32)
    hidden = (jax.nn.silu(gate_val) * up_val).astype(jnp.bfloat16)
    return jnp.dot(hidden, w_down, preferred_element_type=jnp.float32)


def gather_group(block, count):
    copies = jnp.broadcast_to(block[None], (count,) + block.shape)
    return lax.all_to_all(copies, GROUP, 0, 0)


def plain_local(
    tokens,
    rec_state,
    norm_gain,
    w_query,
    w_forget,
    w_input,
    w_outgate,
    lower_bound,
    head_gain,
    w_heads_out,
    mixer_gain,
    w_gate,
    w_up,
    w_down,
):
    kv_count = lax.axis_size("kv")
    tp_count = lax.axis_size("tp")
    kv_index = lax.axis_index("kv")
    tp_index = lax.axis_index("tp")
    group_count = kv_count * tp_count
    row_count = tokens.shape[0]
    seq_count = rec_state.shape[0]
    model_width = norm_gain.shape[0]
    col_block = model_width // kv_count
    tok_float = tokens.astype(jnp.float32)
    other = lax.ppermute(tokens, "tp", [(i, (i + 1) % tp_count) for i in range(tp_count)])
    low = jnp.where(tp_index == 0, tokens, other)
    high = jnp.where(tp_index == 0, other, tokens)
    own_cols = jnp.concatenate([low, high], axis=1).astype(jnp.float32)
    squares = jnp.sum(own_cols * own_cols, axis=1)
    gain_block = lax.dynamic_slice_in_dim(norm_gain, kv_index * col_block, col_block, 0)
    scaled = (own_cols * gain_block).astype(jnp.bfloat16)
    partial = [
        jnp.dot(scaled, weight, preferred_element_type=jnp.float32)
        for weight in (w_query, w_forget, w_input, w_outgate)
    ]
    local_width = w_query.shape[1]
    partial.append(jnp.broadcast_to(squares[:, None], (row_count, 128)))
    sent = jnp.concatenate(partial, axis=1).reshape(kv_count, seq_count, -1)
    projected = jnp.sum(lax.all_to_all(sent, "kv", 0, 0), axis=0)
    my_squares = projected[:, 4 * local_width]
    row_scale = lax.rsqrt(my_squares / model_width + epsilon)[:, None]
    query_pre = row_scale * projected[:, :local_width]
    forget_pre = row_scale * projected[:, local_width : 2 * local_width]
    value_in = row_scale * projected[:, 2 * local_width : 3 * local_width]
    gate_pre = row_scale * projected[:, 3 * local_width : 4 * local_width]
    forget = lower_bound + (1.0 - lower_bound) * jax.nn.sigmoid(forget_pre)
    key_in = 1.0 - forget
    query_act = jax.nn.silu(query_pre)
    head_count = rec_state.shape[1]
    shaped = (seq_count, head_count, HEAD_DIM)
    forget = forget.reshape(shaped)
    key_in = key_in.reshape(shaped)
    value_in = value_in.reshape(shaped)
    query_act = query_act.reshape(shaped)
    new_state = forget[:, :, :, None] * rec_state + key_in[:, :, :, None] * value_in[:, :, None, :]
    head_out = jnp.sum(query_act[:, :, :, None] * new_state, axis=2)
    head_out = head_out * lax.rsqrt(jnp.mean(head_out * head_out, axis=2, keepdims=True) + epsilon)
    head_out = head_out * head_gain.reshape(head_count, HEAD_DIM)
    gated = (head_out.reshape(seq_count, local_width) * jax.nn.silu(gate_pre)).astype(jnp.bfloat16)
    every_head = gather_group(gated, group_count)
    every_head = every_head.reshape(kv_count, tp_count, seq_count, local_width)
    every_head = every_head.transpose(0, 2, 1, 3).reshape(
        kv_count * seq_count, tp_count * local_width
    )
    mixed_add = jnp.dot(every_head, w_heads_out, preferred_element_type=jnp.float32)
    mixed = (tok_float + mixed_add).astype(jnp.bfloat16)
    gathered = gather_group(mixed, group_count).transpose(1, 0, 2).reshape(row_count, model_width)
    terms = channel_mixer(gathered, mixer_gain, w_gate, w_up, w_down)
    out_block = model_width // group_count
    blocked = terms.astype(jnp.bfloat16).reshape(row_count, group_count, out_block)
    blocked = blocked.transpose(1, 0, 2)
    down_sum = jnp.sum(lax.all_to_all(blocked, GROUP, 0, 0).astype(jnp.float32), axis=0)
    result = (mixed.astype(jnp.float32) + down_sum).astype(jnp.bfloat16)
    return (result, new_state)


def choose(*args):
    tokens, rec_state = args[0], args[1]
    w_heads_out, w_gate = args[9], args[11]
    aligned = all(size % LANES == 0 for size in (tokens.shape[1], w_gate.shape[1]))
    small = lax.axis_size("tp") == 2 and lax.axis_size("kv") in (2, 4)
    if aligned and small and rec_state.shape[0] == 1:
        return local(*args)
    return plain_local(*args)


def solution(mesh):
    placed = (
        P("dp", ("kv", "tp")),
        P(("dp", "kv"), "tp", None, None),
        P(),
        P("kv", "tp"),
        P("kv", "tp"),
        P("kv", "tp"),
        P("kv", "tp"),
        P("tp"),
        P("tp"),
        P(None, ("kv", "tp")),
        P(),
        P(None, ("kv", "tp")),
        P(None, ("kv", "tp")),
        P(("kv", "tp"), None),
    )
    return jax.shard_map(
        choose,
        mesh=mesh,
        in_specs=placed,
        out_specs=(P("dp", ("kv", "tp")), P(("dp", "kv"), "tp", None, None)),
        check_vma=False,
    )
```

```python
import jax
import jax.numpy as jnp
from jax import lax
from jax.experimental import pallas as pl
from jax.experimental.pallas import tpu as pltpu
from jax.sharding import PartitionSpec as P

HEAD_DIM = 128
LANES = 128


epsilon = 1e-06
GROUP = ("kv", "tp")
VMEM = pl.BlockSpec(memory_space=pltpu.VMEM)
HBM = pl.BlockSpec(memory_space=pltpu.HBM)


LONG = pl.CostEstimate(flops=10**11, bytes_accessed=10**4, transcendentals=0)
SHORT = pl.CostEstimate(flops=10**7, bytes_accessed=10**4, transcendentals=0)


def resident(array):
    return pltpu.with_memory_space_constraint(array, pltpu.VMEM)


def call(
    body, outs, *args, streamed=(), scratch=(), out_specs=None, limit=6 * 2**20, cost=SHORT
):
    return pl.pallas_call(
        body,
        out_shape=outs,
        in_specs=[VMEM] * len(args) + [HBM] * len(streamed),
        out_specs=out_specs or jax.tree.map(lambda _: VMEM, outs),
        scratch_shapes=scratch,
        compiler_params=pltpu.CompilerParams(vmem_limit_bytes=limit),
        cost_estimate=cost,
    )(*args, *[pltpu.with_memory_space_constraint(w, pltpu.HBM) for w in streamed])


def chip_order(kv_count):
    return [*range(2, kv_count), 1]


def silu(v):
    return v / (1.0 + jnp.exp(-v))


def start_body(
    tokens, norm_gain, w_query, w_forget, w_input, w_outgate,
    own, squares, other_gain, rest, held, held_tokens, held_gain, sems,
):
    half = held.shape[1]
    tp_index, base = lax.axis_index("tp"), lax.axis_index("kv") * 2 * half
    mine = pl.multiple_of(tp_index * half, LANES)
    theirs = pl.multiple_of((1 - tp_index) * half, LANES)
    weights = (w_query, w_forget, w_input, w_outgate)
    moves = [
        (tokens, held_tokens),
        (norm_gain.at[:, pl.ds(pl.multiple_of(base + mine, LANES), half)], held_gain),
        *[(w.at[pl.ds(mine, half), :], held.at[i]) for i, w in enumerate(weights)],
        (norm_gain.at[:, pl.ds(pl.multiple_of(base + theirs, LANES), half)], other_gain),
        *[(w.at[pl.ds(theirs, half), :], rest.at[i]) for i, w in enumerate(weights)],
    ]
    copies = [pltpu.make_async_copy(src, dst, sems.at[i]) for i, (src, dst) in enumerate(moves)]
    for copy in copies:
        copy.start()
    copies[0].wait()
    copies[1].wait()
    cols = held_tokens[...].astype(jnp.float32)
    squares[...] = jnp.broadcast_to(
        jnp.sum(cols * cols, axis=1, keepdims=True), (cols.shape[0], LANES)
    )
    scaled = (cols * held_gain[...]).astype(jnp.bfloat16)
    for i in range(len(weights)):
        copies[2 + i].wait()
        own[i] = jnp.dot(scaled, held[i], preferred_element_type=jnp.float32)
    for copy in copies[2 + len(weights) :]:
        copy.wait()


def project_body(other, own, own_squares, other_gain, rest, kept, *sent_and_scratch):
    *sent, every = sent_and_scratch
    kv_index = lax.axis_index("kv")
    cols = other[...].astype(jnp.float32)
    squares = own_squares[...] + jnp.sum(cols * cols, axis=1, keepdims=True)
    scaled = (cols * other_gain[...]).astype(jnp.bfloat16)
    row = 0
    for i in range(rest.shape[0]):
        product = own[i] + jnp.dot(scaled, rest[i], preferred_element_type=jnp.float32)
        for at in range(0, product.shape[1], LANES):
            every[:, row, :] = product[:, at : at + LANES]
            row += 1
    for at in range(row, every.shape[1]):
        every[:, at, :] = squares
    kept[...] = every[kv_index]
    for j, out in zip(chip_order(len(sent) + 1), sent):
        block = every[kv_index ^ j]
        high = block[row:].astype(jnp.bfloat16).astype(jnp.float32)
        wide = jnp.concatenate([block[:row], high, block[row:] - high], axis=0)
        out[...] = wide.astype(jnp.bfloat16)


def recur_body(model_width, arrived, *refs):
    kept, *received = refs[: arrived + 1]
    rec_state, lower_bound, head_gain, new_state, gated = refs[arrived + 1 :]
    heads = rec_state.shape[0]
    row = 4 * heads
    total = kept[:row]
    squares = kept[row : row + 8]
    for block in received:
        wide = block[...].astype(jnp.float32)
        total = total + wide[:row]
        squares = squares + wide[row : row + 8] + wide[row + 8 : row + 16]
    row_scale = lax.rsqrt(squares[:1] / model_width + epsilon)
    query_pre = row_scale * total[:heads]
    forget_pre = row_scale * total[heads : 2 * heads]
    value_in = row_scale * total[2 * heads : 3 * heads]
    gate_pre = row_scale * total[3 * heads : 4 * heads]
    bound = lower_bound[...]
    forget = bound + (1.0 - bound) / (1.0 + jnp.exp(-forget_pre))
    key_in = 1.0 - forget
    query_act = silu(query_pre)
    forget_t = forget.T
    key_t = key_in.T
    query_t = query_act.T
    rows = []
    for h in range(heads):
        fresh = (
            forget_t[:, h : h + 1] * rec_state[h]
            + key_t[:, h : h + 1] * value_in[h : h + 1, :]
        )
        new_state[h] = fresh
        rows.append(jnp.sum(query_t[:, h : h + 1] * fresh, axis=0, keepdims=True))
    head_out = jnp.concatenate(rows, axis=0)
    head_out = head_out * lax.rsqrt(
        jnp.mean(head_out * head_out, axis=1, keepdims=True) + epsilon
    )
    rounded = (head_out * head_gain[...] * silu(gate_pre)).astype(jnp.bfloat16)
    gated[...] = rounded.astype(jnp.float32)


def pair_body(own, other, out):
    first = lax.axis_index("tp") == 0
    left = own[...].astype(jnp.float32)
    right = other[...].astype(jnp.float32)
    low, high = jnp.where(first, left, right), jnp.where(first, right, left)
    out[...] = jnp.concatenate([low, high], axis=0).astype(out.dtype).reshape(out.shape)


def heads_body(*refs):
    *blocks, w_heads_out, tokens, mixed, every = refs
    kv_index = lax.axis_index("kv")
    for j, block in zip([0, *reversed(chip_order(len(blocks)))], blocks):
        every[kv_index ^ j] = block[...].astype(jnp.float32)
    left = jnp.concatenate([every[:, h, :] for h in range(every.shape[1])], axis=1)
    added = jnp.dot(
        left.astype(jnp.bfloat16), w_heads_out[...], preferred_element_type=jnp.float32
    )
    mixed[...] = (tokens[...].astype(jnp.float32) + added).astype(jnp.bfloat16)


def mixer_block(j, block, mixer_gain, w_gate, w_up):
    depth = block.shape[0] * block.shape[2]
    start = pl.multiple_of((lax.axis_index("kv") ^ j) * depth, LANES)
    cols = jnp.concatenate([block[t] for t in range(block.shape[0])], axis=1)
    cols = cols.astype(jnp.float32)
    squares = jnp.sum(cols * cols, axis=1, keepdims=True)
    gained = (cols * mixer_gain[:, pl.ds(start, depth)]).astype(jnp.bfloat16)
    return (
        jnp.dot(gained, w_gate[pl.ds(start, depth), :], preferred_element_type=jnp.float32),
        jnp.dot(gained, w_up[pl.ds(start, depth), :], preferred_element_type=jnp.float32),
        squares,
    )


def mixer_own_body(
    block, mixer_gain, w_gate, w_up, w_down, new_state, gate, up, squares, state_out, sem
):
    leave = pltpu.make_async_copy(new_state, state_out, sem)
    leave.start()
    gate[...], up[...], summed = mixer_block(0, block, mixer_gain, w_gate, w_up)
    squares[...] = jnp.broadcast_to(summed, squares.shape)
    leave.wait()


def mixer_next_body(
    j, gate_in, up_in, squares_in, block, mixer_gain, w_gate, w_up, w_down, gate, up, squares
):
    more_gate, more_up, more = mixer_block(j, block, mixer_gain, w_gate, w_up)
    gate[...] = gate_in[...] + more_gate
    up[...] = up_in[...] + more_up
    squares[...] = squares_in[...] + more


def down_block(hidden, w_down, chip, core, width):
    start = pl.multiple_of((chip * 2 + core) * width, LANES)
    return jnp.dot(hidden, w_down[:, pl.ds(start, width)], preferred_element_type=jnp.float32)


def mixer_body(*refs):
    gate, up, squares, *blocks = refs[:-6]
    mixer_gain, w_gate, w_up, w_down, hidden, passed = refs[-6:]
    gate_val, up_val, total = gate[...], up[...], squares[:, :1]
    for j, block in zip(reversed(chip_order(lax.axis_size("kv"))), blocks):
        more_gate, more_up, more = mixer_block(j, block, mixer_gain, w_gate, w_up)
        gate_val, up_val, total = gate_val + more_gate, up_val + more_up, total + more
    scale = lax.rsqrt(total / w_gate.shape[0] + epsilon)
    gate_val, up_val = scale * gate_val, scale * up_val
    active = (silu(gate_val) * up_val).astype(jnp.bfloat16)
    hidden[...] = active
    kv_index, tp_index = lax.axis_index("kv"), lax.axis_index("tp")
    for j in range(passed.shape[0]):
        core = 1 - tp_index if j == 0 else tp_index
        passed[j] = down_block(active, w_down, kv_index ^ j, core, passed.shape[2]).astype(
            jnp.bfloat16
        )


def down_body(hidden, w_down, sums):
    kv_index, tp_index = lax.axis_index("kv"), lax.axis_index("tp")
    for j in range(sums.shape[0]):
        core = tp_index if j == 0 else 1 - tp_index
        sums[j] = down_block(hidden[...], w_down, kv_index ^ j, core, sums.shape[2])


def chip_sum_body(sums, passed, mixed, base, *sent):
    base[...] = mixed[...].astype(jnp.float32) + sums[0] + passed[0].astype(jnp.float32)
    for j, out in zip(chip_order(sums.shape[0]), sent):
        out[...] = (sums[j] + passed[j].astype(jnp.float32)).astype(jnp.bfloat16)


def result_body(base, *refs):
    *received, out = refs
    total = base[...]
    for block in received:
        total = total + block[...].astype(jnp.float32)
    out[...] = total.astype(jnp.bfloat16)


def local(
    tokens,
    rec_state,
    norm_gain,
    w_query,
    w_forget,
    w_input,
    w_outgate,
    lower_bound,
    head_gain,
    w_heads_out,
    mixer_gain,
    w_gate,
    w_up,
    w_down,
):
    kv_count = lax.axis_size("kv")
    tp_count = lax.axis_size("tp")
    group_count = kv_count * tp_count
    row_count, own_width = tokens.shape
    heads = rec_state.shape[1]
    model_width = norm_gain.shape[0]
    shape = jax.ShapeDtypeStruct
    others = chip_order(kv_count)
    other = lax.ppermute(tokens, "tp", [(i, (i + 1) % tp_count) for i in range(tp_count)])
    weights = (w_query, w_forget, w_input, w_outgate)
    half_shape = (4, own_width, w_query.shape[1])
    own, squares, other_gain, rest = call(
        start_body,
        (
            shape((4, row_count, w_query.shape[1]), jnp.float32),
            shape((row_count, LANES), jnp.float32),
            pltpu.VMEM((1, own_width), jnp.float32),
            pltpu.VMEM(half_shape, w_query.dtype),
        ),
        streamed=(tokens, norm_gain[None], *weights),
        scratch=[
            pltpu.VMEM(half_shape, w_query.dtype),
            pltpu.VMEM(tokens.shape, tokens.dtype),
            pltpu.VMEM((1, own_width), jnp.float32),
            pltpu.SemaphoreType.DMA((3 + 2 * len(weights),)),
        ],
        limit=12 * 2**20,
    )
    rows = 4 * heads
    kept, *sent = call(
        project_body,
        (
            shape((rows + 8, LANES), jnp.float32),
            *[shape((rows + 16, LANES), jnp.bfloat16)] * (kv_count - 1),
        ),
        other,
        own,
        squares,
        resident(other_gain),
        resident(rest),
        scratch=[pltpu.VMEM((row_count, rows + 8, LANES), jnp.float32)],
        cost=LONG,
    )
    received = [
        lax.ppermute(block, "kv", [(i, i ^ j) for i in range(kv_count)])
        for j, block in zip(others, sent)
    ]
    new_state, gated = call(
        lambda *refs: recur_body(model_width, len(received), *refs),
        (
            pltpu.VMEM(rec_state.shape[1:], jnp.float32),
            shape((heads, HEAD_DIM), jnp.float32),
        ),
        kept,
        *received,
        resident(rec_state[0]),
        lower_bound.reshape(heads, HEAD_DIM),
        head_gain.reshape(heads, HEAD_DIM),
        cost=LONG,
    )

    def swapped(block):
        return lax.ppermute(block, "tp", [(0, 1), (1, 0)])

    def crossed(block, j):
        return lax.ppermute(block, GROUP, [(i, i ^ (2 * j + 1)) for i in range(group_count)])

    def gather(block):
        blocks = {j: crossed(block, j) for j in range(1, kv_count)}
        return [blocks[j] for j in reversed(others)]

    pair = call(
        pair_body, shape((2 * heads, HEAD_DIM), jnp.bfloat16), gated, swapped(gated)
    )
    mixed = call(
        heads_body,
        shape((row_count, own_width), jnp.bfloat16),
        pair,
        *gather(pair),
        resident(w_heads_out),
        tokens,
        scratch=[pltpu.VMEM((kv_count, 2 * heads, HEAD_DIM), jnp.float32)],
    )
    pair = call(
        pair_body, shape((2, row_count, own_width), jnp.bfloat16), mixed, swapped(mixed)
    )
    *blocks, first = gather(pair)
    gain = mixer_gain[None]
    w_gate, w_up, w_down = resident(w_gate), resident(w_up), resident(w_down)
    width = w_gate.shape[1]
    product_shapes = (
        shape((row_count, width), jnp.float32),
        shape((row_count, width), jnp.float32),
        shape((row_count, LANES), jnp.float32),
    )
    *products, new_state = call(
        mixer_own_body,
        (*product_shapes, pltpu.HBM(new_state.shape, jnp.float32)),
        pair,
        gain,
        w_gate,
        w_up,
        w_down,
        resident(new_state),
        out_specs=(VMEM, VMEM, VMEM, HBM),
        scratch=[pltpu.SemaphoreType.DMA],
    )
    if blocks:
        products = call(
            lambda *refs: mixer_next_body(others[0], *refs),
            product_shapes,
            *products,
            first,
            gain,
            w_gate,
            w_up,
            w_down,
        )
    else:
        blocks = [first]
    hidden, passed = call(
        mixer_body,
        (
            shape((row_count, width), jnp.bfloat16),
            shape((kv_count, row_count, own_width), jnp.bfloat16),
        ),
        *products,
        *blocks,
        gain,
        w_gate,
        w_up,
        w_down,
    )
    passed = swapped(passed)
    sums = call(down_body, shape(passed.shape, jnp.float32), hidden, w_down)
    base, *sent = call(
        chip_sum_body,
        (
            shape(mixed.shape, jnp.float32),
            *[shape(mixed.shape, jnp.bfloat16)] * (kv_count - 1),
        ),
        sums,
        passed,
        mixed,
    )
    result = call(
        result_body,
        shape(mixed.shape, jnp.bfloat16),
        base,
        *[crossed(block, j) for j, block in zip(others, sent)],
    )
    return (result, new_state[None])


def channel_mixer(whole_rows, mixer_gain, w_gate, w_up, w_down):
    rows_float = whole_rows.astype(jnp.float32)
    mixer_scale = lax.rsqrt(jnp.mean(rows_float * rows_float, axis=1, keepdims=True) + epsilon)
    normed = (rows_float * mixer_scale * mixer_gain).astype(jnp.bfloat16)
    gate_val = jnp.dot(normed, w_gate, preferred_element_type=jnp.float32)
    up_val = jnp.dot(normed, w_up, preferred_element_type=jnp.float32)
    hidden = (jax.nn.silu(gate_val) * up_val).astype(jnp.bfloat16)
    return jnp.dot(hidden, w_down, preferred_element_type=jnp.float32)


def gather_group(block, count):
    copies = jnp.broadcast_to(block[None], (count,) + block.shape)
    return lax.all_to_all(copies, GROUP, 0, 0)


def plain_local(
    tokens,
    rec_state,
    norm_gain,
    w_query,
    w_forget,
    w_input,
    w_outgate,
    lower_bound,
    head_gain,
    w_heads_out,
    mixer_gain,
    w_gate,
    w_up,
    w_down,
):
    kv_count = lax.axis_size("kv")
    tp_count = lax.axis_size("tp")
    kv_index = lax.axis_index("kv")
    tp_index = lax.axis_index("tp")
    group_count = kv_count * tp_count
    row_count = tokens.shape[0]
    seq_count = rec_state.shape[0]
    model_width = norm_gain.shape[0]
    col_block = model_width // kv_count
    tok_float = tokens.astype(jnp.float32)
    other = lax.ppermute(tokens, "tp", [(i, (i + 1) % tp_count) for i in range(tp_count)])
    low = jnp.where(tp_index == 0, tokens, other)
    high = jnp.where(tp_index == 0, other, tokens)
    own_cols = jnp.concatenate([low, high], axis=1).astype(jnp.float32)
    squares = jnp.sum(own_cols * own_cols, axis=1)
    gain_block = lax.dynamic_slice_in_dim(norm_gain, kv_index * col_block, col_block, 0)
    scaled = (own_cols * gain_block).astype(jnp.bfloat16)
    partial = [
        jnp.dot(scaled, weight, preferred_element_type=jnp.float32)
        for weight in (w_query, w_forget, w_input, w_outgate)
    ]
    local_width = w_query.shape[1]
    partial.append(jnp.broadcast_to(squares[:, None], (row_count, 128)))
    sent = jnp.concatenate(partial, axis=1).reshape(kv_count, seq_count, -1)
    projected = jnp.sum(lax.all_to_all(sent, "kv", 0, 0), axis=0)
    my_squares = projected[:, 4 * local_width]
    row_scale = lax.rsqrt(my_squares / model_width + epsilon)[:, None]
    query_pre = row_scale * projected[:, :local_width]
    forget_pre = row_scale * projected[:, local_width : 2 * local_width]
    value_in = row_scale * projected[:, 2 * local_width : 3 * local_width]
    gate_pre = row_scale * projected[:, 3 * local_width : 4 * local_width]
    forget = lower_bound + (1.0 - lower_bound) * jax.nn.sigmoid(forget_pre)
    key_in = 1.0 - forget
    query_act = jax.nn.silu(query_pre)
    head_count = rec_state.shape[1]
    shaped = (seq_count, head_count, HEAD_DIM)
    forget = forget.reshape(shaped)
    key_in = key_in.reshape(shaped)
    value_in = value_in.reshape(shaped)
    query_act = query_act.reshape(shaped)
    new_state = forget[:, :, :, None] * rec_state + key_in[:, :, :, None] * value_in[:, :, None, :]
    head_out = jnp.sum(query_act[:, :, :, None] * new_state, axis=2)
    head_out = head_out * lax.rsqrt(jnp.mean(head_out * head_out, axis=2, keepdims=True) + epsilon)
    head_out = head_out * head_gain.reshape(head_count, HEAD_DIM)
    gated = (head_out.reshape(seq_count, local_width) * jax.nn.silu(gate_pre)).astype(jnp.bfloat16)
    every_head = gather_group(gated, group_count)
    every_head = every_head.reshape(kv_count, tp_count, seq_count, local_width)
    every_head = every_head.transpose(0, 2, 1, 3).reshape(
        kv_count * seq_count, tp_count * local_width
    )
    mixed_add = jnp.dot(every_head, w_heads_out, preferred_element_type=jnp.float32)
    mixed = (tok_float + mixed_add).astype(jnp.bfloat16)
    gathered = gather_group(mixed, group_count).transpose(1, 0, 2).reshape(row_count, model_width)
    terms = channel_mixer(gathered, mixer_gain, w_gate, w_up, w_down)
    out_block = model_width // group_count
    blocked = terms.astype(jnp.bfloat16).reshape(row_count, group_count, out_block)
    blocked = blocked.transpose(1, 0, 2)
    down_sum = jnp.sum(lax.all_to_all(blocked, GROUP, 0, 0).astype(jnp.float32), axis=0)
    result = (mixed.astype(jnp.float32) + down_sum).astype(jnp.bfloat16)
    return (result, new_state)


def choose(*args):
    tokens, rec_state = args[0], args[1]
    w_heads_out, w_gate = args[9], args[11]
    aligned = all(size % LANES == 0 for size in (tokens.shape[1], w_gate.shape[1]))
    small = lax.axis_size("tp") == 2 and lax.axis_size("kv") in (2, 4)
    if aligned and small and rec_state.shape[0] == 1:
        return local(*args)
    return plain_local(*args)


def solution(mesh):
    placed = (
        P("dp", ("kv", "tp")),
        P(("dp", "kv"), "tp", None, None),
        P(),
        P("kv", "tp"),
        P("kv", "tp"),
        P("kv", "tp"),
        P("kv", "tp"),
        P("tp"),
        P("tp"),
        P(None, ("kv", "tp")),
        P(),
        P(None, ("kv", "tp")),
        P(None, ("kv", "tp")),
        P(("kv", "tp"), None),
    )
    return jax.shard_map(
        choose,
        mesh=mesh,
        in_specs=placed,
        out_specs=(P("dp", ("kv", "tp")), P(("dp", "kv"), "tp", None, None)),
        check_vma=False,
    )
```

```python
import jax
import jax.numpy as jnp
from jax import lax
from jax.experimental import pallas as pl
from jax.experimental.pallas import tpu as pltpu
from jax.sharding import PartitionSpec as P

HEAD_DIM = 128
LANES = 128


epsilon = 1e-06
GROUP = ("kv", "tp")
VMEM = pl.BlockSpec(memory_space=pltpu.VMEM)
HBM = pl.BlockSpec(memory_space=pltpu.HBM)


LONG = pl.CostEstimate(flops=10**11, bytes_accessed=10**4, transcendentals=0)
SHORT = pl.CostEstimate(flops=10**7, bytes_accessed=10**4, transcendentals=0)


def resident(array):
    return pltpu.with_memory_space_constraint(array, pltpu.VMEM)


def call(
    body, outs, *args, streamed=(), scratch=(), out_specs=None, limit=6 * 2**20, cost=SHORT
):
    return pl.pallas_call(
        body,
        out_shape=outs,
        in_specs=[VMEM] * len(args) + [HBM] * len(streamed),
        out_specs=out_specs or jax.tree.map(lambda _: VMEM, outs),
        scratch_shapes=scratch,
        compiler_params=pltpu.CompilerParams(vmem_limit_bytes=limit),
        cost_estimate=cost,
    )(*args, *[pltpu.with_memory_space_constraint(w, pltpu.HBM) for w in streamed])


def chip_order(kv_count):
    return [*range(2, kv_count), 1]


def silu(v):
    return v / (1.0 + jnp.exp(-v))


def start_body(
    tokens, norm_gain, w_query, w_forget, w_input, w_outgate,
    own, squares, other_gain, rest, held, held_tokens, held_gain, sems,
):
    half = held.shape[1]
    tp_index, base = lax.axis_index("tp"), lax.axis_index("kv") * 2 * half
    mine = pl.multiple_of(tp_index * half, LANES)
    theirs = pl.multiple_of((1 - tp_index) * half, LANES)
    weights = (w_query, w_forget, w_input, w_outgate)
    moves = [
        (tokens, held_tokens),
        (norm_gain.at[:, pl.ds(pl.multiple_of(base + mine, LANES), half)], held_gain),
        *[(w.at[pl.ds(mine, half), :], held.at[i]) for i, w in enumerate(weights)],
        (norm_gain.at[:, pl.ds(pl.multiple_of(base + theirs, LANES), half)], other_gain),
        *[(w.at[pl.ds(theirs, half), :], rest.at[i]) for i, w in enumerate(weights)],
    ]
    copies = [pltpu.make_async_copy(src, dst, sems.at[i]) for i, (src, dst) in enumerate(moves)]
    for copy in copies:
        copy.start()
    copies[0].wait()
    copies[1].wait()
    cols = held_tokens[...].astype(jnp.float32)
    squares[...] = jnp.broadcast_to(
        jnp.sum(cols * cols, axis=1, keepdims=True), (cols.shape[0], LANES)
    )
    scaled = (cols * held_gain[...]).astype(jnp.bfloat16)
    for i in range(len(weights)):
        copies[2 + i].wait()
        own[i] = jnp.dot(scaled, held[i], preferred_element_type=jnp.float32)
    for copy in copies[2 + len(weights) :]:
        copy.wait()


def project_body(other, own, own_squares, other_gain, rest, kept, *sent_and_scratch):
    *sent, every = sent_and_scratch
    kv_index = lax.axis_index("kv")
    cols = other[...].astype(jnp.float32)
    squares = own_squares[...] + jnp.sum(cols * cols, axis=1, keepdims=True)
    scaled = (cols * other_gain[...]).astype(jnp.bfloat16)
    row = 0
    for i in range(rest.shape[0]):
        product = own[i] + jnp.dot(scaled, rest[i], preferred_element_type=jnp.float32)
        for at in range(0, product.shape[1], LANES):
            every[:, row, :] = product[:, at : at + LANES]
            row += 1
    for at in range(row, every.shape[1]):
        every[:, at, :] = squares
    kept[...] = every[kv_index]
    for j, out in zip(chip_order(len(sent) + 1), sent):
        block = every[kv_index ^ j]
        high = block[row:].astype(jnp.bfloat16).astype(jnp.float32)
        wide = jnp.concatenate([block[:row], high, block[row:] - high], axis=0)
        out[...] = wide.astype(jnp.bfloat16)


def recur_body(model_width, arrived, *refs):
    kept, *received = refs[: arrived + 1]
    rec_state, lower_bound, head_gain, new_state, gated = refs[arrived + 1 :]
    heads = rec_state.shape[0]
    row = 4 * heads
    total = kept[:row]
    squares = kept[row : row + 8]
    for block in received:
        wide = block[...].astype(jnp.float32)
        total = total + wide[:row]
        squares = squares + wide[row : row + 8] + wide[row + 8 : row + 16]
    row_scale = lax.rsqrt(squares[:1] / model_width + epsilon)
    query_pre = row_scale * total[:heads]
    forget_pre = row_scale * total[heads : 2 * heads]
    value_in = row_scale * total[2 * heads : 3 * heads]
    gate_pre = row_scale * total[3 * heads : 4 * heads]
    bound = lower_bound[...]
    forget = bound + (1.0 - bound) / (1.0 + jnp.exp(-forget_pre))
    key_in = 1.0 - forget
    query_act = silu(query_pre)
    forget_t = forget.T
    key_t = key_in.T
    query_t = query_act.T
    rows = []
    for h in range(heads):
        fresh = (
            forget_t[:, h : h + 1] * rec_state[h]
            + key_t[:, h : h + 1] * value_in[h : h + 1, :]
        )
        new_state[h] = fresh
        rows.append(jnp.sum(query_t[:, h : h + 1] * fresh, axis=0, keepdims=True))
    head_out = jnp.concatenate(rows, axis=0)
    head_out = head_out * lax.rsqrt(
        jnp.mean(head_out * head_out, axis=1, keepdims=True) + epsilon
    )
    rounded = (head_out * head_gain[...] * silu(gate_pre)).astype(jnp.bfloat16)
    gated[...] = rounded.astype(jnp.float32)


def pair_body(own, other, out):
    first = lax.axis_index("tp") == 0
    left = own[...].astype(jnp.float32)
    right = other[...].astype(jnp.float32)
    low, high = jnp.where(first, left, right), jnp.where(first, right, left)
    out[...] = jnp.concatenate([low, high], axis=0).astype(out.dtype).reshape(out.shape)


def heads_body(*refs):
    *blocks, w_own, w_other, tokens, other_tokens, mixed, own_mixed, every = refs
    kv_index = lax.axis_index("kv")
    for j, block in zip([0, *reversed(chip_order(len(blocks)))], blocks):
        every[kv_index ^ j] = block[...].astype(jnp.float32)
    left = jnp.concatenate([every[:, h, :] for h in range(every.shape[1])], axis=1)
    left = left.astype(jnp.bfloat16)
    tp_index = lax.axis_index("tp")
    for place, weight, start in (
        (tp_index, w_own, tokens),
        (1 - tp_index, w_other, other_tokens),
    ):
        added = jnp.dot(left, weight[...], preferred_element_type=jnp.float32)
        rounded = (start[...].astype(jnp.float32) + added).astype(jnp.bfloat16)
        mixed[place] = rounded
        if weight is w_own:
            own_mixed[...] = rounded


def mixer_block(j, block, mixer_gain, w_gate, w_up):
    depth = block.shape[0] * block.shape[2]
    start = pl.multiple_of((lax.axis_index("kv") ^ j) * depth, LANES)
    cols = jnp.concatenate([block[t] for t in range(block.shape[0])], axis=1)
    cols = cols.astype(jnp.float32)
    squares = jnp.sum(cols * cols, axis=1, keepdims=True)
    gained = (cols * mixer_gain[:, pl.ds(start, depth)]).astype(jnp.bfloat16)
    return (
        jnp.dot(gained, w_gate[pl.ds(start, depth), :], preferred_element_type=jnp.float32),
        jnp.dot(gained, w_up[pl.ds(start, depth), :], preferred_element_type=jnp.float32),
        squares,
    )


def mixer_own_body(
    block, mixer_gain, w_gate, w_up, w_down, new_state, gate, up, squares, state_out, sem
):
    leave = pltpu.make_async_copy(new_state, state_out, sem)
    leave.start()
    gate[...], up[...], summed = mixer_block(0, block, mixer_gain, w_gate, w_up)
    squares[...] = jnp.broadcast_to(summed, squares.shape)
    leave.wait()


def mixer_next_body(
    j, gate_in, up_in, squares_in, block, mixer_gain, w_gate, w_up, w_down, gate, up, squares
):
    more_gate, more_up, more = mixer_block(j, block, mixer_gain, w_gate, w_up)
    gate[...] = gate_in[...] + more_gate
    up[...] = up_in[...] + more_up
    squares[...] = squares_in[...] + more


def down_block(hidden, w_down, chip, core, width):
    start = pl.multiple_of((chip * 2 + core) * width, LANES)
    return jnp.dot(hidden, w_down[:, pl.ds(start, width)], preferred_element_type=jnp.float32)


def mixer_body(*refs):
    gate, up, squares, *blocks = refs[:-6]
    mixer_gain, w_gate, w_up, w_down, hidden, passed = refs[-6:]
    gate_val, up_val, total = gate[...], up[...], squares[:, :1]
    for j, block in zip(reversed(chip_order(lax.axis_size("kv"))), blocks):
        more_gate, more_up, more = mixer_block(j, block, mixer_gain, w_gate, w_up)
        gate_val, up_val, total = gate_val + more_gate, up_val + more_up, total + more
    scale = lax.rsqrt(total / w_gate.shape[0] + epsilon)
    gate_val, up_val = scale * gate_val, scale * up_val
    active = (silu(gate_val) * up_val).astype(jnp.bfloat16)
    hidden[...] = active
    kv_index, tp_index = lax.axis_index("kv"), lax.axis_index("tp")
    for j in range(passed.shape[0]):
        core = 1 - tp_index if j == 0 else tp_index
        passed[j] = down_block(active, w_down, kv_index ^ j, core, passed.shape[2]).astype(
            jnp.bfloat16
        )


def down_body(hidden, w_down, sums):
    kv_index, tp_index = lax.axis_index("kv"), lax.axis_index("tp")
    for j in range(sums.shape[0]):
        core = tp_index if j == 0 else 1 - tp_index
        sums[j] = down_block(hidden[...], w_down, kv_index ^ j, core, sums.shape[2])


def chip_sum_body(sums, passed, mixed, base, *sent):
    base[...] = mixed[...].astype(jnp.float32) + sums[0] + passed[0].astype(jnp.float32)
    for j, out in zip(chip_order(sums.shape[0]), sent):
        out[...] = (sums[j] + passed[j].astype(jnp.float32)).astype(jnp.bfloat16)


def result_body(base, *refs):
    *received, out = refs
    total = base[...]
    for block in received:
        total = total + block[...].astype(jnp.float32)
    out[...] = total.astype(jnp.bfloat16)


def local(
    tokens,
    rec_state,
    norm_gain,
    w_query,
    w_forget,
    w_input,
    w_outgate,
    lower_bound,
    head_gain,
    w_heads_out,
    mixer_gain,
    w_gate,
    w_up,
    w_down,
):
    kv_count = lax.axis_size("kv")
    tp_count = lax.axis_size("tp")
    group_count = kv_count * tp_count
    row_count, own_width = tokens.shape
    heads = rec_state.shape[1]
    model_width = norm_gain.shape[0]
    shape = jax.ShapeDtypeStruct
    others = chip_order(kv_count)

    def swapped(block):
        return lax.ppermute(block, "tp", [(0, 1), (1, 0)])

    other = swapped(tokens)
    weights = (w_query, w_forget, w_input, w_outgate)
    half_shape = (4, own_width, w_query.shape[1])
    own, squares, other_gain, rest = call(
        start_body,
        (
            shape((4, row_count, w_query.shape[1]), jnp.float32),
            shape((row_count, LANES), jnp.float32),
            pltpu.VMEM((1, own_width), jnp.float32),
            pltpu.VMEM(half_shape, w_query.dtype),
        ),
        streamed=(tokens, norm_gain[None], *weights),
        scratch=[
            pltpu.VMEM(half_shape, w_query.dtype),
            pltpu.VMEM(tokens.shape, tokens.dtype),
            pltpu.VMEM((1, own_width), jnp.float32),
            pltpu.SemaphoreType.DMA((3 + 2 * len(weights),)),
        ],
        limit=12 * 2**20,
    )
    rows = 4 * heads
    kept, *sent = call(
        project_body,
        (
            shape((rows + 8, LANES), jnp.float32),
            *[shape((rows + 16, LANES), jnp.bfloat16)] * (kv_count - 1),
        ),
        other,
        own,
        squares,
        resident(other_gain),
        resident(rest),
        scratch=[pltpu.VMEM((row_count, rows + 8, LANES), jnp.float32)],
        cost=LONG,
    )
    w_early, kept = lax.optimization_barrier((w_heads_out, kept))
    w_other = swapped(w_early)
    received = [
        lax.ppermute(block, "kv", [(i, i ^ j) for i in range(kv_count)])
        for j, block in zip(others, sent)
    ]
    new_state, gated = call(
        lambda *refs: recur_body(model_width, len(received), *refs),
        (
            pltpu.VMEM(rec_state.shape[1:], jnp.float32),
            shape((heads, HEAD_DIM), jnp.float32),
        ),
        kept,
        *received,
        resident(rec_state[0]),
        lower_bound.reshape(heads, HEAD_DIM),
        head_gain.reshape(heads, HEAD_DIM),
        cost=LONG,
    )

    def crossed(block, j):
        return lax.ppermute(block, GROUP, [(i, i ^ (2 * j + 1)) for i in range(group_count)])

    def gather(block):
        blocks = {j: crossed(block, j) for j in range(1, kv_count)}
        return [blocks[j] for j in reversed(others)]

    pair = call(
        pair_body, shape((2 * heads, HEAD_DIM), jnp.bfloat16), gated, swapped(gated)
    )
    pair, mixed = call(
        heads_body,
        (
            shape((2, row_count, own_width), jnp.bfloat16),
            shape((row_count, own_width), jnp.bfloat16),
        ),
        pair,
        *gather(pair),
        resident(w_heads_out),
        resident(w_other),
        tokens,
        other,
        scratch=[pltpu.VMEM((kv_count, 2 * heads, HEAD_DIM), jnp.float32)],
    )
    *blocks, first = gather(pair)
    gain = mixer_gain[None]
    w_gate, w_up, w_down = resident(w_gate), resident(w_up), resident(w_down)
    width = w_gate.shape[1]
    product_shapes = (
        shape((row_count, width), jnp.float32),
        shape((row_count, width), jnp.float32),
        shape((row_count, LANES), jnp.float32),
    )
    *products, new_state = call(
        mixer_own_body,
        (*product_shapes, pltpu.HBM(new_state.shape, jnp.float32)),
        pair,
        gain,
        w_gate,
        w_up,
        w_down,
        resident(new_state),
        out_specs=(VMEM, VMEM, VMEM, HBM),
        scratch=[pltpu.SemaphoreType.DMA],
    )
    if blocks:
        products = call(
            lambda *refs: mixer_next_body(others[0], *refs),
            product_shapes,
            *products,
            first,
            gain,
            w_gate,
            w_up,
            w_down,
        )
    else:
        blocks = [first]
    hidden, passed = call(
        mixer_body,
        (
            shape((row_count, width), jnp.bfloat16),
            shape((kv_count, row_count, own_width), jnp.bfloat16),
        ),
        *products,
        *blocks,
        gain,
        w_gate,
        w_up,
        w_down,
    )
    passed = swapped(passed)
    sums = call(down_body, shape(passed.shape, jnp.float32), hidden, w_down)
    base, *sent = call(
        chip_sum_body,
        (
            shape(mixed.shape, jnp.float32),
            *[shape(mixed.shape, jnp.bfloat16)] * (kv_count - 1),
        ),
        sums,
        passed,
        mixed,
    )
    result = call(
        result_body,
        shape(mixed.shape, jnp.bfloat16),
        base,
        *[crossed(block, j) for j, block in zip(others, sent)],
    )
    return (result, new_state[None])


def channel_mixer(whole_rows, mixer_gain, w_gate, w_up, w_down):
    rows_float = whole_rows.astype(jnp.float32)
    mixer_scale = lax.rsqrt(jnp.mean(rows_float * rows_float, axis=1, keepdims=True) + epsilon)
    normed = (rows_float * mixer_scale * mixer_gain).astype(jnp.bfloat16)
    gate_val = jnp.dot(normed, w_gate, preferred_element_type=jnp.float32)
    up_val = jnp.dot(normed, w_up, preferred_element_type=jnp.float32)
    hidden = (jax.nn.silu(gate_val) * up_val).astype(jnp.bfloat16)
    return jnp.dot(hidden, w_down, preferred_element_type=jnp.float32)


def gather_group(block, count):
    copies = jnp.broadcast_to(block[None], (count,) + block.shape)
    return lax.all_to_all(copies, GROUP, 0, 0)


def plain_local(
    tokens,
    rec_state,
    norm_gain,
    w_query,
    w_forget,
    w_input,
    w_outgate,
    lower_bound,
    head_gain,
    w_heads_out,
    mixer_gain,
    w_gate,
    w_up,
    w_down,
):
    kv_count = lax.axis_size("kv")
    tp_count = lax.axis_size("tp")
    kv_index = lax.axis_index("kv")
    tp_index = lax.axis_index("tp")
    group_count = kv_count * tp_count
    row_count = tokens.shape[0]
    seq_count = rec_state.shape[0]
    model_width = norm_gain.shape[0]
    col_block = model_width // kv_count
    tok_float = tokens.astype(jnp.float32)
    other = lax.ppermute(tokens, "tp", [(i, (i + 1) % tp_count) for i in range(tp_count)])
    low = jnp.where(tp_index == 0, tokens, other)
    high = jnp.where(tp_index == 0, other, tokens)
    own_cols = jnp.concatenate([low, high], axis=1).astype(jnp.float32)
    squares = jnp.sum(own_cols * own_cols, axis=1)
    gain_block = lax.dynamic_slice_in_dim(norm_gain, kv_index * col_block, col_block, 0)
    scaled = (own_cols * gain_block).astype(jnp.bfloat16)
    partial = [
        jnp.dot(scaled, weight, preferred_element_type=jnp.float32)
        for weight in (w_query, w_forget, w_input, w_outgate)
    ]
    local_width = w_query.shape[1]
    partial.append(jnp.broadcast_to(squares[:, None], (row_count, 128)))
    sent = jnp.concatenate(partial, axis=1).reshape(kv_count, seq_count, -1)
    projected = jnp.sum(lax.all_to_all(sent, "kv", 0, 0), axis=0)
    my_squares = projected[:, 4 * local_width]
    row_scale = lax.rsqrt(my_squares / model_width + epsilon)[:, None]
    query_pre = row_scale * projected[:, :local_width]
    forget_pre = row_scale * projected[:, local_width : 2 * local_width]
    value_in = row_scale * projected[:, 2 * local_width : 3 * local_width]
    gate_pre = row_scale * projected[:, 3 * local_width : 4 * local_width]
    forget = lower_bound + (1.0 - lower_bound) * jax.nn.sigmoid(forget_pre)
    key_in = 1.0 - forget
    query_act = jax.nn.silu(query_pre)
    head_count = rec_state.shape[1]
    shaped = (seq_count, head_count, HEAD_DIM)
    forget = forget.reshape(shaped)
    key_in = key_in.reshape(shaped)
    value_in = value_in.reshape(shaped)
    query_act = query_act.reshape(shaped)
    new_state = forget[:, :, :, None] * rec_state + key_in[:, :, :, None] * value_in[:, :, None, :]
    head_out = jnp.sum(query_act[:, :, :, None] * new_state, axis=2)
    head_out = head_out * lax.rsqrt(jnp.mean(head_out * head_out, axis=2, keepdims=True) + epsilon)
    head_out = head_out * head_gain.reshape(head_count, HEAD_DIM)
    gated = (head_out.reshape(seq_count, local_width) * jax.nn.silu(gate_pre)).astype(jnp.bfloat16)
    every_head = gather_group(gated, group_count)
    every_head = every_head.reshape(kv_count, tp_count, seq_count, local_width)
    every_head = every_head.transpose(0, 2, 1, 3).reshape(
        kv_count * seq_count, tp_count * local_width
    )
    mixed_add = jnp.dot(every_head, w_heads_out, preferred_element_type=jnp.float32)
    mixed = (tok_float + mixed_add).astype(jnp.bfloat16)
    gathered = gather_group(mixed, group_count).transpose(1, 0, 2).reshape(row_count, model_width)
    terms = channel_mixer(gathered, mixer_gain, w_gate, w_up, w_down)
    out_block = model_width // group_count
    blocked = terms.astype(jnp.bfloat16).reshape(row_count, group_count, out_block)
    blocked = blocked.transpose(1, 0, 2)
    down_sum = jnp.sum(lax.all_to_all(blocked, GROUP, 0, 0).astype(jnp.float32), axis=0)
    result = (mixed.astype(jnp.float32) + down_sum).astype(jnp.bfloat16)
    return (result, new_state)


def choose(*args):
    tokens, rec_state = args[0], args[1]
    w_heads_out, w_gate = args[9], args[11]
    aligned = all(size % LANES == 0 for size in (tokens.shape[1], w_gate.shape[1]))
    small = lax.axis_size("tp") == 2 and lax.axis_size("kv") in (2, 4)
    if aligned and small and rec_state.shape[0] == 1:
        return local(*args)
    return plain_local(*args)


def solution(mesh):
    placed = (
        P("dp", ("kv", "tp")),
        P(("dp", "kv"), "tp", None, None),
        P(),
        P("kv", "tp"),
        P("kv", "tp"),
        P("kv", "tp"),
        P("kv", "tp"),
        P("tp"),
        P("tp"),
        P(None, ("kv", "tp")),
        P(),
        P(None, ("kv", "tp")),
        P(None, ("kv", "tp")),
        P(("kv", "tp"), None),
    )
    return jax.shard_map(
        choose,
        mesh=mesh,
        in_specs=placed,
        out_specs=(P("dp", ("kv", "tp")), P(("dp", "kv"), "tp", None, None)),
        check_vma=False,
    )
```

```python
import jax
import jax.numpy as jnp
from jax import lax
from jax.experimental import pallas as pl
from jax.experimental.pallas import tpu as pltpu
from jax.sharding import PartitionSpec as P

HEAD_DIM = 128
LANES = 128


epsilon = 1e-06
GROUP = ("kv", "tp")
VMEM = pl.BlockSpec(memory_space=pltpu.VMEM)
HBM = pl.BlockSpec(memory_space=pltpu.HBM)


LONG = pl.CostEstimate(flops=10**11, bytes_accessed=10**4, transcendentals=0)
SHORT = pl.CostEstimate(flops=10**7, bytes_accessed=10**4, transcendentals=0)


def resident(array):
    return pltpu.with_memory_space_constraint(array, pltpu.VMEM)


def call(
    body, outs, *args, streamed=(), scratch=(), out_specs=None, limit=6 * 2**20, cost=SHORT
):
    return pl.pallas_call(
        body,
        out_shape=outs,
        in_specs=[VMEM] * len(args) + [HBM] * len(streamed),
        out_specs=out_specs or jax.tree.map(lambda _: VMEM, outs),
        scratch_shapes=scratch,
        compiler_params=pltpu.CompilerParams(vmem_limit_bytes=limit),
        cost_estimate=cost,
    )(*args, *[pltpu.with_memory_space_constraint(w, pltpu.HBM) for w in streamed])


def chip_order(kv_count):
    return [*range(2, kv_count), 1]


def silu(v):
    return v / (1.0 + jnp.exp(-v))


def start_body(
    tokens, norm_gain, w_query, w_forget, w_input, w_outgate,
    own, squares, other_gain, rest, held, held_tokens, held_gain, sems,
):
    half = held.shape[1]
    tp_index, base = lax.axis_index("tp"), lax.axis_index("kv") * 2 * half
    mine = pl.multiple_of(tp_index * half, LANES)
    theirs = pl.multiple_of((1 - tp_index) * half, LANES)
    weights = (w_query, w_forget, w_input, w_outgate)
    moves = [
        (tokens, held_tokens),
        (norm_gain.at[:, pl.ds(pl.multiple_of(base + mine, LANES), half)], held_gain),
        *[(w.at[pl.ds(mine, half), :], held.at[i]) for i, w in enumerate(weights)],
        (norm_gain.at[:, pl.ds(pl.multiple_of(base + theirs, LANES), half)], other_gain),
        *[(w.at[pl.ds(theirs, half), :], rest.at[i]) for i, w in enumerate(weights)],
    ]
    copies = [pltpu.make_async_copy(src, dst, sems.at[i]) for i, (src, dst) in enumerate(moves)]
    for copy in copies:
        copy.start()
    copies[0].wait()
    copies[1].wait()
    cols = held_tokens[...].astype(jnp.float32)
    squares[...] = jnp.broadcast_to(
        jnp.sum(cols * cols, axis=1, keepdims=True), (cols.shape[0], LANES)
    )
    scaled = (cols * held_gain[...]).astype(jnp.bfloat16)
    for i in range(len(weights)):
        copies[2 + i].wait()
        own[i] = jnp.dot(scaled, held[i], preferred_element_type=jnp.float32)
    for copy in copies[2 + len(weights) :]:
        copy.wait()


def project_body(other, own, own_squares, other_gain, rest, kept, *sent_and_scratch):
    *sent, every = sent_and_scratch
    kv_index = lax.axis_index("kv")
    cols = other[...].astype(jnp.float32)
    squares = own_squares[...] + jnp.sum(cols * cols, axis=1, keepdims=True)
    scaled = (cols * other_gain[...]).astype(jnp.bfloat16)
    row = 0
    for i in range(rest.shape[0]):
        product = own[i] + jnp.dot(scaled, rest[i], preferred_element_type=jnp.float32)
        for at in range(0, product.shape[1], LANES):
            every[:, row, :] = product[:, at : at + LANES]
            row += 1
    for at in range(row, every.shape[1]):
        every[:, at, :] = squares
    kept[...] = every[kv_index]
    for j, out in zip(chip_order(len(sent) + 1), sent):
        block = every[kv_index ^ j]
        high = block[row:].astype(jnp.bfloat16).astype(jnp.float32)
        wide = jnp.concatenate([block[:row], high, block[row:] - high], axis=0)
        out[...] = wide.astype(jnp.bfloat16)


def recur_body(model_width, arrived, *refs):
    kept, *received = refs[: arrived + 1]
    rec_state, lower_bound, head_gain, gates, gated = refs[arrived + 1 :]
    heads = rec_state.shape[0]
    row = 4 * heads
    total = kept[:row]
    squares = kept[row : row + 8]
    for block in received:
        wide = block[...].astype(jnp.float32)
        total = total + wide[:row]
        squares = squares + wide[row : row + 8] + wide[row + 8 : row + 16]
    row_scale = lax.rsqrt(squares[:1] / model_width + epsilon)
    query_pre = row_scale * total[:heads]
    forget_pre = row_scale * total[heads : 2 * heads]
    value_in = row_scale * total[2 * heads : 3 * heads]
    gate_pre = row_scale * total[3 * heads : 4 * heads]
    bound = lower_bound[...]
    forget = bound + (1.0 - bound) / (1.0 + jnp.exp(-forget_pre))
    key_in = 1.0 - forget
    query_act = silu(query_pre)
    gates[0], gates[1], gates[2] = forget, key_in, value_in
    read_t = (query_act * forget).T
    rows = [
        jnp.sum(read_t[:, h : h + 1] * rec_state[h], axis=0, keepdims=True)
        for h in range(heads)
    ]
    fresh = jnp.sum(query_act * key_in, axis=1, keepdims=True) * value_in
    head_out = jnp.concatenate(rows, axis=0) + fresh
    head_out = head_out * lax.rsqrt(
        jnp.mean(head_out * head_out, axis=1, keepdims=True) + epsilon
    )
    rounded = (head_out * head_gain[...] * silu(gate_pre)).astype(jnp.bfloat16)
    gated[...] = rounded.astype(jnp.float32)


def state_body(gates, rec_state, new_state):
    forget_t = gates[0].T
    key_t = gates[1].T
    value_in = gates[2]
    for h in range(rec_state.shape[0]):
        new_state[h] = (
            forget_t[:, h : h + 1] * rec_state[h]
            + key_t[:, h : h + 1] * value_in[h : h + 1, :]
        )


def pair_body(own, other, out):
    first = lax.axis_index("tp") == 0
    left = own[...].astype(jnp.float32)
    right = other[...].astype(jnp.float32)
    low, high = jnp.where(first, left, right), jnp.where(first, right, left)
    out[...] = jnp.concatenate([low, high], axis=0).astype(out.dtype).reshape(out.shape)


def heads_body(*refs):
    *blocks, w_own, w_other, tokens, other_tokens, mixed, own_mixed, every = refs
    kv_index = lax.axis_index("kv")
    for j, block in zip([0, *reversed(chip_order(len(blocks)))], blocks):
        every[kv_index ^ j] = block[...].astype(jnp.float32)
    left = jnp.concatenate([every[:, h, :] for h in range(every.shape[1])], axis=1)
    left = left.astype(jnp.bfloat16)
    tp_index = lax.axis_index("tp")
    for place, weight, start in (
        (tp_index, w_own, tokens),
        (1 - tp_index, w_other, other_tokens),
    ):
        added = jnp.dot(left, weight[...], preferred_element_type=jnp.float32)
        rounded = (start[...].astype(jnp.float32) + added).astype(jnp.bfloat16)
        mixed[place] = rounded
        if weight is w_own:
            own_mixed[...] = rounded


def mixer_block(j, block, mixer_gain, w_gate, w_up):
    depth = block.shape[0] * block.shape[2]
    start = pl.multiple_of((lax.axis_index("kv") ^ j) * depth, LANES)
    cols = jnp.concatenate([block[t] for t in range(block.shape[0])], axis=1)
    cols = cols.astype(jnp.float32)
    squares = jnp.sum(cols * cols, axis=1, keepdims=True)
    gained = (cols * mixer_gain[:, pl.ds(start, depth)]).astype(jnp.bfloat16)
    return (
        jnp.dot(gained, w_gate[pl.ds(start, depth), :], preferred_element_type=jnp.float32),
        jnp.dot(gained, w_up[pl.ds(start, depth), :], preferred_element_type=jnp.float32),
        squares,
    )


def mixer_own_body(
    block, mixer_gain, w_gate, w_up, w_down, new_state, gate, up, squares, state_out, sem
):
    leave = pltpu.make_async_copy(new_state, state_out, sem)
    leave.start()
    gate[...], up[...], summed = mixer_block(0, block, mixer_gain, w_gate, w_up)
    squares[...] = jnp.broadcast_to(summed, squares.shape)
    leave.wait()


def mixer_next_body(
    j, gate_in, up_in, squares_in, block, mixer_gain, w_gate, w_up, w_down, gate, up, squares
):
    more_gate, more_up, more = mixer_block(j, block, mixer_gain, w_gate, w_up)
    gate[...] = gate_in[...] + more_gate
    up[...] = up_in[...] + more_up
    squares[...] = squares_in[...] + more


def down_block(hidden, w_down, chip, core, width):
    start = pl.multiple_of((chip * 2 + core) * width, LANES)
    return jnp.dot(hidden, w_down[:, pl.ds(start, width)], preferred_element_type=jnp.float32)


def mixer_body(*refs):
    gate, up, squares, *blocks = refs[:-6]
    mixer_gain, w_gate, w_up, w_down, hidden, passed = refs[-6:]
    gate_val, up_val, total = gate[...], up[...], squares[:, :1]
    for j, block in zip(reversed(chip_order(lax.axis_size("kv"))), blocks):
        more_gate, more_up, more = mixer_block(j, block, mixer_gain, w_gate, w_up)
        gate_val, up_val, total = gate_val + more_gate, up_val + more_up, total + more
    scale = lax.rsqrt(total / w_gate.shape[0] + epsilon)
    gate_val, up_val = scale * gate_val, scale * up_val
    active = (silu(gate_val) * up_val).astype(jnp.bfloat16)
    hidden[...] = active
    kv_index, tp_index = lax.axis_index("kv"), lax.axis_index("tp")
    for j in range(passed.shape[0]):
        core = 1 - tp_index if j == 0 else tp_index
        passed[j] = down_block(active, w_down, kv_index ^ j, core, passed.shape[2]).astype(
            jnp.bfloat16
        )


def down_body(hidden, w_down, sums):
    kv_index, tp_index = lax.axis_index("kv"), lax.axis_index("tp")
    for j in range(sums.shape[0]):
        core = tp_index if j == 0 else 1 - tp_index
        sums[j] = down_block(hidden[...], w_down, kv_index ^ j, core, sums.shape[2])


def chip_sum_body(sums, passed, mixed, base, *sent):
    base[...] = mixed[...].astype(jnp.float32) + sums[0] + passed[0].astype(jnp.float32)
    for j, out in zip(chip_order(sums.shape[0]), sent):
        out[...] = (sums[j] + passed[j].astype(jnp.float32)).astype(jnp.bfloat16)


def result_body(base, *refs):
    *received, out = refs
    total = base[...]
    for block in received:
        total = total + block[...].astype(jnp.float32)
    out[...] = total.astype(jnp.bfloat16)


def local(
    tokens,
    rec_state,
    norm_gain,
    w_query,
    w_forget,
    w_input,
    w_outgate,
    lower_bound,
    head_gain,
    w_heads_out,
    mixer_gain,
    w_gate,
    w_up,
    w_down,
):
    kv_count = lax.axis_size("kv")
    tp_count = lax.axis_size("tp")
    group_count = kv_count * tp_count
    row_count, own_width = tokens.shape
    heads = rec_state.shape[1]
    model_width = norm_gain.shape[0]
    shape = jax.ShapeDtypeStruct
    others = chip_order(kv_count)

    def swapped(block):
        return lax.ppermute(block, "tp", [(0, 1), (1, 0)])

    other = swapped(tokens)
    weights = (w_query, w_forget, w_input, w_outgate)
    half_shape = (4, own_width, w_query.shape[1])
    own, squares, other_gain, rest = call(
        start_body,
        (
            shape((4, row_count, w_query.shape[1]), jnp.float32),
            shape((row_count, LANES), jnp.float32),
            pltpu.VMEM((1, own_width), jnp.float32),
            pltpu.VMEM(half_shape, w_query.dtype),
        ),
        streamed=(tokens, norm_gain[None], *weights),
        scratch=[
            pltpu.VMEM(half_shape, w_query.dtype),
            pltpu.VMEM(tokens.shape, tokens.dtype),
            pltpu.VMEM((1, own_width), jnp.float32),
            pltpu.SemaphoreType.DMA((3 + 2 * len(weights),)),
        ],
        limit=12 * 2**20,
    )
    rows = 4 * heads
    kept, *sent = call(
        project_body,
        (
            shape((rows + 8, LANES), jnp.float32),
            *[shape((rows + 16, LANES), jnp.bfloat16)] * (kv_count - 1),
        ),
        other,
        own,
        squares,
        resident(other_gain),
        resident(rest),
        scratch=[pltpu.VMEM((row_count, rows + 8, LANES), jnp.float32)],
        cost=LONG,
    )
    w_early, kept = lax.optimization_barrier((w_heads_out, kept))
    w_other = swapped(w_early)
    received = [
        lax.ppermute(block, "kv", [(i, i ^ j) for i in range(kv_count)])
        for j, block in zip(others, sent)
    ]
    state = resident(rec_state[0])
    gates, gated = call(
        lambda *refs: recur_body(model_width, len(received), *refs),
        (
            shape((3, heads, HEAD_DIM), jnp.float32),
            shape((heads, HEAD_DIM), jnp.float32),
        ),
        kept,
        *received,
        state,
        lower_bound.reshape(heads, HEAD_DIM),
        head_gain.reshape(heads, HEAD_DIM),
        cost=LONG,
    )

    def crossed(block, j):
        return lax.ppermute(block, GROUP, [(i, i ^ (2 * j + 1)) for i in range(group_count)])

    new_state = call(
        state_body, pltpu.VMEM(rec_state.shape[1:], jnp.float32), gates, state
    )

    def gather(block):
        blocks = {j: crossed(block, j) for j in range(1, kv_count)}
        return [blocks[j] for j in reversed(others)]

    pair = call(
        pair_body, shape((2 * heads, HEAD_DIM), jnp.bfloat16), gated, swapped(gated)
    )
    *arrived, new_state = lax.optimization_barrier((*gather(pair), new_state))
    pair, mixed = call(
        heads_body,
        (
            shape((2, row_count, own_width), jnp.bfloat16),
            shape((row_count, own_width), jnp.bfloat16),
        ),
        pair,
        *arrived,
        resident(w_heads_out),
        resident(w_other),
        tokens,
        other,
        scratch=[pltpu.VMEM((kv_count, 2 * heads, HEAD_DIM), jnp.float32)],
    )
    *blocks, first = gather(pair)
    gain = mixer_gain[None]
    w_gate, w_up, w_down = resident(w_gate), resident(w_up), resident(w_down)
    width = w_gate.shape[1]
    product_shapes = (
        shape((row_count, width), jnp.float32),
        shape((row_count, width), jnp.float32),
        shape((row_count, LANES), jnp.float32),
    )
    *products, new_state = call(
        mixer_own_body,
        (*product_shapes, pltpu.HBM(new_state.shape, jnp.float32)),
        pair,
        gain,
        w_gate,
        w_up,
        w_down,
        resident(new_state),
        out_specs=(VMEM, VMEM, VMEM, HBM),
        scratch=[pltpu.SemaphoreType.DMA],
    )
    if blocks:
        products = call(
            lambda *refs: mixer_next_body(others[0], *refs),
            product_shapes,
            *products,
            first,
            gain,
            w_gate,
            w_up,
            w_down,
        )
    else:
        blocks = [first]
    hidden, passed = call(
        mixer_body,
        (
            shape((row_count, width), jnp.bfloat16),
            shape((kv_count, row_count, own_width), jnp.bfloat16),
        ),
        *products,
        *blocks,
        gain,
        w_gate,
        w_up,
        w_down,
    )
    passed = swapped(passed)
    sums = call(down_body, shape(passed.shape, jnp.float32), hidden, w_down)
    base, *sent = call(
        chip_sum_body,
        (
            shape(mixed.shape, jnp.float32),
            *[shape(mixed.shape, jnp.bfloat16)] * (kv_count - 1),
        ),
        sums,
        passed,
        mixed,
    )
    result = call(
        result_body,
        shape(mixed.shape, jnp.bfloat16),
        base,
        *[crossed(block, j) for j, block in zip(others, sent)],
    )
    return (result, new_state[None])


def channel_mixer(whole_rows, mixer_gain, w_gate, w_up, w_down):
    rows_float = whole_rows.astype(jnp.float32)
    mixer_scale = lax.rsqrt(jnp.mean(rows_float * rows_float, axis=1, keepdims=True) + epsilon)
    normed = (rows_float * mixer_scale * mixer_gain).astype(jnp.bfloat16)
    gate_val = jnp.dot(normed, w_gate, preferred_element_type=jnp.float32)
    up_val = jnp.dot(normed, w_up, preferred_element_type=jnp.float32)
    hidden = (jax.nn.silu(gate_val) * up_val).astype(jnp.bfloat16)
    return jnp.dot(hidden, w_down, preferred_element_type=jnp.float32)


def gather_group(block, count):
    copies = jnp.broadcast_to(block[None], (count,) + block.shape)
    return lax.all_to_all(copies, GROUP, 0, 0)


def plain_local(
    tokens,
    rec_state,
    norm_gain,
    w_query,
    w_forget,
    w_input,
    w_outgate,
    lower_bound,
    head_gain,
    w_heads_out,
    mixer_gain,
    w_gate,
    w_up,
    w_down,
):
    kv_count = lax.axis_size("kv")
    tp_count = lax.axis_size("tp")
    kv_index = lax.axis_index("kv")
    tp_index = lax.axis_index("tp")
    group_count = kv_count * tp_count
    row_count = tokens.shape[0]
    seq_count = rec_state.shape[0]
    model_width = norm_gain.shape[0]
    col_block = model_width // kv_count
    tok_float = tokens.astype(jnp.float32)
    other = lax.ppermute(tokens, "tp", [(i, (i + 1) % tp_count) for i in range(tp_count)])
    low = jnp.where(tp_index == 0, tokens, other)
    high = jnp.where(tp_index == 0, other, tokens)
    own_cols = jnp.concatenate([low, high], axis=1).astype(jnp.float32)
    squares = jnp.sum(own_cols * own_cols, axis=1)
    gain_block = lax.dynamic_slice_in_dim(norm_gain, kv_index * col_block, col_block, 0)
    scaled = (own_cols * gain_block).astype(jnp.bfloat16)
    partial = [
        jnp.dot(scaled, weight, preferred_element_type=jnp.float32)
        for weight in (w_query, w_forget, w_input, w_outgate)
    ]
    local_width = w_query.shape[1]
    partial.append(jnp.broadcast_to(squares[:, None], (row_count, 128)))
    sent = jnp.concatenate(partial, axis=1).reshape(kv_count, seq_count, -1)
    projected = jnp.sum(lax.all_to_all(sent, "kv", 0, 0), axis=0)
    my_squares = projected[:, 4 * local_width]
    row_scale = lax.rsqrt(my_squares / model_width + epsilon)[:, None]
    query_pre = row_scale * projected[:, :local_width]
    forget_pre = row_scale * projected[:, local_width : 2 * local_width]
    value_in = row_scale * projected[:, 2 * local_width : 3 * local_width]
    gate_pre = row_scale * projected[:, 3 * local_width : 4 * local_width]
    forget = lower_bound + (1.0 - lower_bound) * jax.nn.sigmoid(forget_pre)
    key_in = 1.0 - forget
    query_act = jax.nn.silu(query_pre)
    head_count = rec_state.shape[1]
    shaped = (seq_count, head_count, HEAD_DIM)
    forget = forget.reshape(shaped)
    key_in = key_in.reshape(shaped)
    value_in = value_in.reshape(shaped)
    query_act = query_act.reshape(shaped)
    new_state = forget[:, :, :, None] * rec_state + key_in[:, :, :, None] * value_in[:, :, None, :]
    head_out = jnp.sum(query_act[:, :, :, None] * new_state, axis=2)
    head_out = head_out * lax.rsqrt(jnp.mean(head_out * head_out, axis=2, keepdims=True) + epsilon)
    head_out = head_out * head_gain.reshape(head_count, HEAD_DIM)
    gated = (head_out.reshape(seq_count, local_width) * jax.nn.silu(gate_pre)).astype(jnp.bfloat16)
    every_head = gather_group(gated, group_count)
    every_head = every_head.reshape(kv_count, tp_count, seq_count, local_width)
    every_head = every_head.transpose(0, 2, 1, 3).reshape(
        kv_count * seq_count, tp_count * local_width
    )
    mixed_add = jnp.dot(every_head, w_heads_out, preferred_element_type=jnp.float32)
    mixed = (tok_float + mixed_add).astype(jnp.bfloat16)
    gathered = gather_group(mixed, group_count).transpose(1, 0, 2).reshape(row_count, model_width)
    terms = channel_mixer(gathered, mixer_gain, w_gate, w_up, w_down)
    out_block = model_width // group_count
    blocked = terms.astype(jnp.bfloat16).reshape(row_count, group_count, out_block)
    blocked = blocked.transpose(1, 0, 2)
    down_sum = jnp.sum(lax.all_to_all(blocked, GROUP, 0, 0).astype(jnp.float32), axis=0)
    result = (mixed.astype(jnp.float32) + down_sum).astype(jnp.bfloat16)
    return (result, new_state)


def choose(*args):
    tokens, rec_state = args[0], args[1]
    w_heads_out, w_gate = args[9], args[11]
    aligned = all(size % LANES == 0 for size in (tokens.shape[1], w_gate.shape[1]))
    small = lax.axis_size("tp") == 2 and lax.axis_size("kv") in (2, 4)
    if aligned and small and rec_state.shape[0] == 1:
        return local(*args)
    return plain_local(*args)


def solution(mesh):
    placed = (
        P("dp", ("kv", "tp")),
        P(("dp", "kv"), "tp", None, None),
        P(),
        P("kv", "tp"),
        P("kv", "tp"),
        P("kv", "tp"),
        P("kv", "tp"),
        P("tp"),
        P("tp"),
        P(None, ("kv", "tp")),
        P(),
        P(None, ("kv", "tp")),
        P(None, ("kv", "tp")),
        P(("kv", "tp"), None),
    )
    return jax.shard_map(
        choose,
        mesh=mesh,
        in_specs=placed,
        out_specs=(P("dp", ("kv", "tp")), P(("dp", "kv"), "tp", None, None)),
        check_vma=False,
    )
```

```python
import jax
import jax.numpy as jnp
from jax import lax
from jax.experimental import pallas as pl
from jax.experimental.pallas import tpu as pltpu
from jax.sharding import PartitionSpec as P

HEAD_DIM = 128
LANES = 128


epsilon = 1e-06
GROUP = ("kv", "tp")
VMEM = pl.BlockSpec(memory_space=pltpu.VMEM)
HBM = pl.BlockSpec(memory_space=pltpu.HBM)


LONG = pl.CostEstimate(flops=10**11, bytes_accessed=10**4, transcendentals=0)
SHORT = pl.CostEstimate(flops=10**7, bytes_accessed=10**4, transcendentals=0)


def resident(array):
    return pltpu.with_memory_space_constraint(array, pltpu.VMEM)


def call(
    body, outs, *args, streamed=(), scratch=(), out_specs=None, limit=6 * 2**20, cost=SHORT
):
    return pl.pallas_call(
        body,
        out_shape=outs,
        in_specs=[VMEM] * len(args) + [HBM] * len(streamed),
        out_specs=out_specs or jax.tree.map(lambda _: VMEM, outs),
        scratch_shapes=scratch,
        compiler_params=pltpu.CompilerParams(vmem_limit_bytes=limit),
        cost_estimate=cost,
    )(*args, *[pltpu.with_memory_space_constraint(w, pltpu.HBM) for w in streamed])


def chip_order(kv_count):
    return [*range(2, kv_count), 1]


def silu(v):
    return v / (1.0 + jnp.exp(-v))


def start_body(
    tokens, norm_gain, w_query, w_forget, w_input, w_outgate,
    own, squares, other_gain, rest, held, held_tokens, held_gain, sems,
):
    half = held.shape[1]
    tp_index, base = lax.axis_index("tp"), lax.axis_index("kv") * 2 * half
    mine = pl.multiple_of(tp_index * half, LANES)
    theirs = pl.multiple_of((1 - tp_index) * half, LANES)
    weights = (w_query, w_forget, w_input, w_outgate)
    moves = [
        (tokens, held_tokens),
        (norm_gain.at[:, pl.ds(pl.multiple_of(base + mine, LANES), half)], held_gain),
        *[(w.at[pl.ds(mine, half), :], held.at[i]) for i, w in enumerate(weights)],
        (norm_gain.at[:, pl.ds(pl.multiple_of(base + theirs, LANES), half)], other_gain),
        *[(w.at[pl.ds(theirs, half), :], rest.at[i]) for i, w in enumerate(weights)],
    ]
    copies = [pltpu.make_async_copy(src, dst, sems.at[i]) for i, (src, dst) in enumerate(moves)]
    for i, copy in enumerate(copies):
        copy.start(priority=i % 2)
    copies[0].wait()
    copies[1].wait()
    cols = held_tokens[...].astype(jnp.float32)
    squares[...] = jnp.broadcast_to(
        jnp.sum(cols * cols, axis=1, keepdims=True), (cols.shape[0], LANES)
    )
    scaled = (cols * held_gain[...]).astype(jnp.bfloat16)
    for i in range(len(weights)):
        copies[2 + i].wait()
        own[i] = jnp.dot(scaled, held[i], preferred_element_type=jnp.float32)
    for copy in copies[2 + len(weights) :]:
        copy.wait()


def project_body(other, own, own_squares, other_gain, rest, kept, *sent_and_scratch):
    *sent, every = sent_and_scratch
    kv_index = lax.axis_index("kv")
    cols = other[...].astype(jnp.float32)
    squares = own_squares[...] + jnp.sum(cols * cols, axis=1, keepdims=True)
    scaled = (cols * other_gain[...]).astype(jnp.bfloat16)
    row = 0
    for i in range(rest.shape[0]):
        product = own[i] + jnp.dot(scaled, rest[i], preferred_element_type=jnp.float32)
        for at in range(0, product.shape[1], LANES):
            every[:, row, :] = product[:, at : at + LANES]
            row += 1
    for at in range(row, every.shape[1]):
        every[:, at, :] = squares
    kept[...] = every[kv_index]
    for j, out in zip(chip_order(len(sent) + 1), sent):
        block = every[kv_index ^ j]
        high = block[row:].astype(jnp.bfloat16).astype(jnp.float32)
        wide = jnp.concatenate([block[:row], high, block[row:] - high], axis=0)
        out[...] = wide.astype(jnp.bfloat16)


def recur_body(model_width, arrived, *refs):
    kept, *received = refs[: arrived + 1]
    rec_state, lower_bound, head_gain, gates, gated = refs[arrived + 1 :]
    heads = rec_state.shape[0]
    row = 4 * heads
    total = kept[:row]
    squares = kept[row : row + 8]
    for block in received:
        wide = block[...].astype(jnp.float32)
        total = total + wide[:row]
        squares = squares + wide[row : row + 8] + wide[row + 8 : row + 16]
    row_scale = lax.rsqrt(squares[:1] / model_width + epsilon)
    query_pre = row_scale * total[:heads]
    forget_pre = row_scale * total[heads : 2 * heads]
    value_in = row_scale * total[2 * heads : 3 * heads]
    gate_pre = row_scale * total[3 * heads : 4 * heads]
    bound = lower_bound[...]
    forget = bound + (1.0 - bound) / (1.0 + jnp.exp(-forget_pre))
    key_in = 1.0 - forget
    query_act = silu(query_pre)
    gates[0], gates[1], gates[2] = forget, key_in, value_in
    read_t = (query_act * forget).T
    rows = [
        jnp.sum(read_t[:, h : h + 1] * rec_state[h], axis=0, keepdims=True)
        for h in range(heads)
    ]
    fresh = jnp.sum(query_act * key_in, axis=1, keepdims=True) * value_in
    head_out = jnp.concatenate(rows, axis=0) + fresh
    head_out = head_out * lax.rsqrt(
        jnp.mean(head_out * head_out, axis=1, keepdims=True) + epsilon
    )
    rounded = (head_out * head_gain[...] * silu(gate_pre)).astype(jnp.bfloat16)
    gated[...] = rounded.astype(jnp.float32)


def state_body(gates, rec_state, new_state):
    forget_t = gates[0].T
    key_t = gates[1].T
    value_in = gates[2]
    for h in range(rec_state.shape[0]):
        new_state[h] = (
            forget_t[:, h : h + 1] * rec_state[h]
            + key_t[:, h : h + 1] * value_in[h : h + 1, :]
        )


def pair_body(own, other, out):
    first = lax.axis_index("tp") == 0
    left = own[...].astype(jnp.float32)
    right = other[...].astype(jnp.float32)
    low, high = jnp.where(first, left, right), jnp.where(first, right, left)
    out[...] = jnp.concatenate([low, high], axis=0).astype(out.dtype).reshape(out.shape)


def heads_body(*refs):
    *blocks, w_own, w_other, tokens, other_tokens, mixed, own_mixed, every = refs
    kv_index = lax.axis_index("kv")
    for j, block in zip([0, *reversed(chip_order(len(blocks)))], blocks):
        every[kv_index ^ j] = block[...].astype(jnp.float32)
    left = jnp.concatenate([every[:, h, :] for h in range(every.shape[1])], axis=1)
    left = left.astype(jnp.bfloat16)
    tp_index = lax.axis_index("tp")
    for place, weight, start in (
        (tp_index, w_own, tokens),
        (1 - tp_index, w_other, other_tokens),
    ):
        added = jnp.dot(left, weight[...], preferred_element_type=jnp.float32)
        rounded = (start[...].astype(jnp.float32) + added).astype(jnp.bfloat16)
        mixed[place] = rounded
        if weight is w_own:
            own_mixed[...] = rounded


def mixer_block(j, block, mixer_gain, w_gate, w_up):
    depth = block.shape[0] * block.shape[2]
    start = pl.multiple_of((lax.axis_index("kv") ^ j) * depth, LANES)
    cols = jnp.concatenate([block[t] for t in range(block.shape[0])], axis=1)
    cols = cols.astype(jnp.float32)
    squares = jnp.sum(cols * cols, axis=1, keepdims=True)
    gained = (cols * mixer_gain[:, pl.ds(start, depth)]).astype(jnp.bfloat16)
    return (
        jnp.dot(gained, w_gate[pl.ds(start, depth), :], preferred_element_type=jnp.float32),
        jnp.dot(gained, w_up[pl.ds(start, depth), :], preferred_element_type=jnp.float32),
        squares,
    )


def mixer_own_body(
    block, mixer_gain, w_gate, w_up, w_down, new_state, gate, up, squares, state_out, sem
):
    leave = pltpu.make_async_copy(new_state, state_out, sem)
    leave.start()
    gate[...], up[...], summed = mixer_block(0, block, mixer_gain, w_gate, w_up)
    squares[...] = jnp.broadcast_to(summed, squares.shape)
    leave.wait()


def mixer_next_body(
    j, gate_in, up_in, squares_in, block, mixer_gain, w_gate, w_up, w_down, gate, up, squares
):
    more_gate, more_up, more = mixer_block(j, block, mixer_gain, w_gate, w_up)
    gate[...] = gate_in[...] + more_gate
    up[...] = up_in[...] + more_up
    squares[...] = squares_in[...] + more


def down_block(hidden, w_down, chip, core, width):
    start = pl.multiple_of((chip * 2 + core) * width, LANES)
    return jnp.dot(hidden, w_down[:, pl.ds(start, width)], preferred_element_type=jnp.float32)


def mixer_body(*refs):
    gate, up, squares, *blocks = refs[:-6]
    mixer_gain, w_gate, w_up, w_down, hidden, passed = refs[-6:]
    gate_val, up_val, total = gate[...], up[...], squares[:, :1]
    for j, block in zip(reversed(chip_order(lax.axis_size("kv"))), blocks):
        more_gate, more_up, more = mixer_block(j, block, mixer_gain, w_gate, w_up)
        gate_val, up_val, total = gate_val + more_gate, up_val + more_up, total + more
    scale = lax.rsqrt(total / w_gate.shape[0] + epsilon)
    gate_val, up_val = scale * gate_val, scale * up_val
    active = (silu(gate_val) * up_val).astype(jnp.bfloat16)
    hidden[...] = active
    kv_index, tp_index = lax.axis_index("kv"), lax.axis_index("tp")
    for j in range(passed.shape[0]):
        core = 1 - tp_index if j == 0 else tp_index
        passed[j] = down_block(active, w_down, kv_index ^ j, core, passed.shape[2]).astype(
            jnp.bfloat16
        )


def down_body(hidden, w_down, sums):
    kv_index, tp_index = lax.axis_index("kv"), lax.axis_index("tp")
    for j in range(sums.shape[0]):
        core = tp_index if j == 0 else 1 - tp_index
        sums[j] = down_block(hidden[...], w_down, kv_index ^ j, core, sums.shape[2])


def chip_sum_body(sums, passed, mixed, base, *sent):
    base[...] = mixed[...].astype(jnp.float32) + sums[0] + passed[0].astype(jnp.float32)
    for j, out in zip(reversed(range(1, sums.shape[0])), sent):
        out[...] = (sums[j] + passed[j].astype(jnp.float32)).astype(jnp.bfloat16)


def result_body(base, *refs):
    *received, out = refs
    total = base[...]
    for block in received:
        total = total + block[...].astype(jnp.float32)
    out[...] = total.astype(jnp.bfloat16)


def local(
    tokens,
    rec_state,
    norm_gain,
    w_query,
    w_forget,
    w_input,
    w_outgate,
    lower_bound,
    head_gain,
    w_heads_out,
    mixer_gain,
    w_gate,
    w_up,
    w_down,
):
    kv_count = lax.axis_size("kv")
    tp_count = lax.axis_size("tp")
    group_count = kv_count * tp_count
    row_count, own_width = tokens.shape
    heads = rec_state.shape[1]
    model_width = norm_gain.shape[0]
    shape = jax.ShapeDtypeStruct
    others = chip_order(kv_count)

    def swapped(block):
        return lax.ppermute(block, "tp", [(0, 1), (1, 0)])

    other = swapped(tokens)
    weights = (w_query, w_forget, w_input, w_outgate)
    half_shape = (4, own_width, w_query.shape[1])
    own, squares, other_gain, rest = call(
        start_body,
        (
            shape((4, row_count, w_query.shape[1]), jnp.float32),
            shape((row_count, LANES), jnp.float32),
            pltpu.VMEM((1, own_width), jnp.float32),
            pltpu.VMEM(half_shape, w_query.dtype),
        ),
        streamed=(tokens, norm_gain[None], *weights),
        scratch=[
            pltpu.VMEM(half_shape, w_query.dtype),
            pltpu.VMEM(tokens.shape, tokens.dtype),
            pltpu.VMEM((1, own_width), jnp.float32),
            pltpu.SemaphoreType.DMA((3 + 2 * len(weights),)),
        ],
        limit=12 * 2**20,
    )
    rows = 4 * heads
    kept, *sent = call(
        project_body,
        (
            shape((rows + 8, LANES), jnp.float32),
            *[shape((rows + 16, LANES), jnp.bfloat16)] * (kv_count - 1),
        ),
        other,
        own,
        squares,
        resident(other_gain),
        resident(rest),
        scratch=[pltpu.VMEM((row_count, rows + 8, LANES), jnp.float32)],
        cost=LONG,
    )
    w_early, kept = lax.optimization_barrier((w_heads_out, kept))
    w_other = swapped(w_early)
    received = [
        lax.ppermute(block, "kv", [(i, i ^ j) for i in range(kv_count)])
        for j, block in zip(others, sent)
    ]
    state = resident(rec_state[0])
    gates, gated = call(
        lambda *refs: recur_body(model_width, len(received), *refs),
        (
            shape((3, heads, HEAD_DIM), jnp.float32),
            shape((heads, HEAD_DIM), jnp.float32),
        ),
        kept,
        *received,
        state,
        lower_bound.reshape(heads, HEAD_DIM),
        head_gain.reshape(heads, HEAD_DIM),
        cost=LONG,
    )

    def crossed(block, j):
        return lax.ppermute(block, GROUP, [(i, i ^ (2 * j + 1)) for i in range(group_count)])

    new_state = call(
        state_body, pltpu.VMEM(rec_state.shape[1:], jnp.float32), gates, state
    )

    def gather(block):
        blocks = {j: crossed(block, j) for j in range(1, kv_count)}
        return [blocks[j] for j in reversed(others)]

    pair = call(
        pair_body, shape((2 * heads, HEAD_DIM), jnp.bfloat16), gated, swapped(gated)
    )
    *arrived, new_state = lax.optimization_barrier((*gather(pair), new_state))
    pair, mixed = call(
        heads_body,
        (
            shape((2, row_count, own_width), jnp.bfloat16),
            shape((row_count, own_width), jnp.bfloat16),
        ),
        pair,
        *arrived,
        resident(w_heads_out),
        resident(w_other),
        tokens,
        other,
        scratch=[pltpu.VMEM((kv_count, 2 * heads, HEAD_DIM), jnp.float32)],
    )
    *blocks, first = gather(pair)
    gain = mixer_gain[None]
    w_gate, w_up, w_down = resident(w_gate), resident(w_up), resident(w_down)
    width = w_gate.shape[1]
    product_shapes = (
        shape((row_count, width), jnp.float32),
        shape((row_count, width), jnp.float32),
        shape((row_count, LANES), jnp.float32),
    )
    *products, new_state = call(
        mixer_own_body,
        (*product_shapes, pltpu.HBM(new_state.shape, jnp.float32)),
        pair,
        gain,
        w_gate,
        w_up,
        w_down,
        resident(new_state),
        out_specs=(VMEM, VMEM, VMEM, HBM),
        scratch=[pltpu.SemaphoreType.DMA],
    )
    if blocks:
        products = call(
            lambda *refs: mixer_next_body(others[0], *refs),
            product_shapes,
            *products,
            first,
            gain,
            w_gate,
            w_up,
            w_down,
        )
    else:
        blocks = [first]
    hidden, passed = call(
        mixer_body,
        (
            shape((row_count, width), jnp.bfloat16),
            shape((kv_count, row_count, own_width), jnp.bfloat16),
        ),
        *products,
        *blocks,
        gain,
        w_gate,
        w_up,
        w_down,
    )
    passed = swapped(passed)
    sums = call(down_body, shape(passed.shape, jnp.float32), hidden, w_down)
    base, *sent = call(
        chip_sum_body,
        (
            shape(mixed.shape, jnp.float32),
            *[shape(mixed.shape, jnp.bfloat16)] * (kv_count - 1),
        ),
        sums,
        passed,
        mixed,
    )
    result = call(
        result_body,
        shape(mixed.shape, jnp.bfloat16),
        base,
        *[crossed(block, j) for j, block in zip(reversed(range(1, kv_count)), sent)],
    )
    return (result, new_state[None])


def channel_mixer(whole_rows, mixer_gain, w_gate, w_up, w_down):
    rows_float = whole_rows.astype(jnp.float32)
    mixer_scale = lax.rsqrt(jnp.mean(rows_float * rows_float, axis=1, keepdims=True) + epsilon)
    normed = (rows_float * mixer_scale * mixer_gain).astype(jnp.bfloat16)
    gate_val = jnp.dot(normed, w_gate, preferred_element_type=jnp.float32)
    up_val = jnp.dot(normed, w_up, preferred_element_type=jnp.float32)
    hidden = (jax.nn.silu(gate_val) * up_val).astype(jnp.bfloat16)
    return jnp.dot(hidden, w_down, preferred_element_type=jnp.float32)


def gather_group(block, count):
    copies = jnp.broadcast_to(block[None], (count,) + block.shape)
    return lax.all_to_all(copies, GROUP, 0, 0)


def plain_local(
    tokens,
    rec_state,
    norm_gain,
    w_query,
    w_forget,
    w_input,
    w_outgate,
    lower_bound,
    head_gain,
    w_heads_out,
    mixer_gain,
    w_gate,
    w_up,
    w_down,
):
    kv_count = lax.axis_size("kv")
    tp_count = lax.axis_size("tp")
    kv_index = lax.axis_index("kv")
    tp_index = lax.axis_index("tp")
    group_count = kv_count * tp_count
    row_count = tokens.shape[0]
    seq_count = rec_state.shape[0]
    model_width = norm_gain.shape[0]
    col_block = model_width // kv_count
    tok_float = tokens.astype(jnp.float32)
    other = lax.ppermute(tokens, "tp", [(i, (i + 1) % tp_count) for i in range(tp_count)])
    low = jnp.where(tp_index == 0, tokens, other)
    high = jnp.where(tp_index == 0, other, tokens)
    own_cols = jnp.concatenate([low, high], axis=1).astype(jnp.float32)
    squares = jnp.sum(own_cols * own_cols, axis=1)
    gain_block = lax.dynamic_slice_in_dim(norm_gain, kv_index * col_block, col_block, 0)
    scaled = (own_cols * gain_block).astype(jnp.bfloat16)
    partial = [
        jnp.dot(scaled, weight, preferred_element_type=jnp.float32)
        for weight in (w_query, w_forget, w_input, w_outgate)
    ]
    local_width = w_query.shape[1]
    partial.append(jnp.broadcast_to(squares[:, None], (row_count, 128)))
    sent = jnp.concatenate(partial, axis=1).reshape(kv_count, seq_count, -1)
    projected = jnp.sum(lax.all_to_all(sent, "kv", 0, 0), axis=0)
    my_squares = projected[:, 4 * local_width]
    row_scale = lax.rsqrt(my_squares / model_width + epsilon)[:, None]
    query_pre = row_scale * projected[:, :local_width]
    forget_pre = row_scale * projected[:, local_width : 2 * local_width]
    value_in = row_scale * projected[:, 2 * local_width : 3 * local_width]
    gate_pre = row_scale * projected[:, 3 * local_width : 4 * local_width]
    forget = lower_bound + (1.0 - lower_bound) * jax.nn.sigmoid(forget_pre)
    key_in = 1.0 - forget
    query_act = jax.nn.silu(query_pre)
    head_count = rec_state.shape[1]
    shaped = (seq_count, head_count, HEAD_DIM)
    forget = forget.reshape(shaped)
    key_in = key_in.reshape(shaped)
    value_in = value_in.reshape(shaped)
    query_act = query_act.reshape(shaped)
    new_state = forget[:, :, :, None] * rec_state + key_in[:, :, :, None] * value_in[:, :, None, :]
    head_out = jnp.sum(query_act[:, :, :, None] * new_state, axis=2)
    head_out = head_out * lax.rsqrt(jnp.mean(head_out * head_out, axis=2, keepdims=True) + epsilon)
    head_out = head_out * head_gain.reshape(head_count, HEAD_DIM)
    gated = (head_out.reshape(seq_count, local_width) * jax.nn.silu(gate_pre)).astype(jnp.bfloat16)
    every_head = gather_group(gated, group_count)
    every_head = every_head.reshape(kv_count, tp_count, seq_count, local_width)
    every_head = every_head.transpose(0, 2, 1, 3).reshape(
        kv_count * seq_count, tp_count * local_width
    )
    mixed_add = jnp.dot(every_head, w_heads_out, preferred_element_type=jnp.float32)
    mixed = (tok_float + mixed_add).astype(jnp.bfloat16)
    gathered = gather_group(mixed, group_count).transpose(1, 0, 2).reshape(row_count, model_width)
    terms = channel_mixer(gathered, mixer_gain, w_gate, w_up, w_down)
    out_block = model_width // group_count
    blocked = terms.astype(jnp.bfloat16).reshape(row_count, group_count, out_block)
    blocked = blocked.transpose(1, 0, 2)
    down_sum = jnp.sum(lax.all_to_all(blocked, GROUP, 0, 0).astype(jnp.float32), axis=0)
    result = (mixed.astype(jnp.float32) + down_sum).astype(jnp.bfloat16)
    return (result, new_state)


def choose(*args):
    tokens, rec_state = args[0], args[1]
    w_heads_out, w_gate = args[9], args[11]
    aligned = all(size % LANES == 0 for size in (tokens.shape[1], w_gate.shape[1]))
    small = lax.axis_size("tp") == 2 and lax.axis_size("kv") in (2, 4)
    if aligned and small and rec_state.shape[0] == 1:
        return local(*args)
    return plain_local(*args)


def solution(mesh):
    placed = (
        P("dp", ("kv", "tp")),
        P(("dp", "kv"), "tp", None, None),
        P(),
        P("kv", "tp"),
        P("kv", "tp"),
        P("kv", "tp"),
        P("kv", "tp"),
        P("tp"),
        P("tp"),
        P(None, ("kv", "tp")),
        P(),
        P(None, ("kv", "tp")),
        P(None, ("kv", "tp")),
        P(("kv", "tp"), None),
    )
    return jax.shard_map(
        choose,
        mesh=mesh,
        in_specs=placed,
        out_specs=(P("dp", ("kv", "tp")), P(("dp", "kv"), "tp", None, None)),
        check_vma=False,
    )
```
